256 devices in a mesh: sp: 32 (over z, y), tp: 8 (over x, core).
Axes of the slice: x: 4, y: 4, z: 8, core: 2. Of those that a mesh axis runs over, the one named last changes fastest.
Arguments:
- source: bfloat16 [16384, 2048], P(('sp', 'tp')), may hold values from -6 to 6
- target: bfloat16 [4096, 2048], P(('sp', 'tp')), may hold values from -6 to 6
- source_gain: bfloat16 [2, 2048], replicated, may hold values from 0.099609375 to 1.8984375
- target_gain: bfloat16 [2, 2048], replicated, may hold values from 0.099609375 to 1.8984375
- query_weight: bfloat16 [2, 2048, 1024], P(None, None, 'tp'), may hold values from -0.5 to 0.5
- key_weight: bfloat16 [2, 2048, 1024], P(None, None, 'tp'), may hold values from -0.5 to 0.5
- value_weight: bfloat16 [2, 2048, 1024], P(None, None, 'tp'), may hold values from -0.125 to 0.125
- head_gain: bfloat16 [2, 1024], P(None, 'tp'), may hold values from 0.099609375 to 1.8984375
- out_weight: bfloat16 [2, 1024, 2048], P(None, 'tp'), may hold values from -0.1875 to 0.1875
- mlp_gain: bfloat16 [2048], replicated, may hold values from 0.099609375 to 1.8984375
- gate_weight: bfloat16 [2048, 5632], P(None, 'tp'), may hold values from -0.125 to 0.125
- up_weight: bfloat16 [2048, 5632], P(None, 'tp'), may hold values from -0.125 to 0.125
- down_weight: bfloat16 [5632, 2048], P('tp'), may hold values from -0.078125 to 0.078125
Outputs:
- mixed: bfloat16 [4096, 2048], P(('sp', 'tp'))
The draws below stay inside these ranges and needn't reach their ends.
All inputs are finite; a program needn't handle non-finite values.
Results may differ from the reference program's by a relative error of at most 0.014.
Values may be sent and summed in bfloat16 or wider, within the bound.
A program may use at most 128 MiB of HBM per device.

```python
import jax
import jax.numpy as jnp
from jax import lax

D = 2048
HEADS = 8
HEAD_DIM = 128
FF = 5632
LAYERS = 2
SRC_DEV = 512
QW = 1024
TARGET = 4096
SOURCE = 16384
N_SP = 32


def source_rows(key):
    rows = jax.random.normal(jax.random.fold_in(key, 31), (SOURCE, D), jnp.float32)
    return jnp.clip(rows, -6.0, 6.0)


def draw_source(key, part):
    return source_rows(key).astype(jnp.bfloat16)


def draw_target(key, part):
    rows = jnp.clip(jax.random.normal(jax.random.fold_in(key, 33), (TARGET, D), jnp.float32), -6.0, 6.0)
    return rows.astype(jnp.bfloat16)


def own_noise(key, salt):
    return jax.random.normal(jax.random.fold_in(key, salt), (LAYERS, D, QW), jnp.float32) * D ** (-0.5)


def draw_query_weight(key, part):
    weight = jnp.clip(own_noise(key, 42), -0.5, 0.5)
    return weight.astype(jnp.bfloat16)


def draw_key_weight(key, part):
    weight = jnp.clip(own_noise(key, 43), -0.5, 0.5)
    return weight.astype(jnp.bfloat16)


def level_of(rng, shape, shards, least, high):
    def one(axis_at, blocks):
        draws = jax.random.uniform(jax.random.fold_in(jax.random.fold_in(rng, 6), axis_at), (blocks,), jnp.float32, least / len(shards), high / len(shards))
        return jnp.repeat(jnp.exp(draws), shape[axis_at] // blocks).reshape((-1,) + (1,) * (len(shape) - axis_at - 1))

    loudness = one(*shards[0])
    for cut in shards[1:]:
        loudness = loudness * one(*cut)
    return loudness


def bell_draw(own_key, shape, width, limit, shards=(), dtype=jnp.bfloat16):
    result = jax.random.normal(own_key, shape, jnp.float32) * width
    if len(shards) > 0:
        result = level_of(own_key, shape, shards, -0.22, 0.18) * result
    return jnp.clip(result, min=-limit, max=limit).astype(dtype)


def setup_inputs(seed: int = 0) -> dict:
    splits = jax.random.split(jax.random.key(seed), 14)
    return {
        "source": draw_source(jax.random.fold_in(splits[13], 71), 0),
        "target": draw_target(jax.random.fold_in(splits[13], 71), 0),
        "source_gain": jnp.clip(1.0 + 0.18 * jax.random.normal(splits[2], (LAYERS, D), jnp.float32), 0.099609375, 1.8984375).astype(jnp.bfloat16),
        "target_gain": jnp.clip(1.0 + 0.18 * jax.random.normal(splits[3], (LAYERS, D), jnp.float32), 0.099609375, 1.8984375).astype(jnp.bfloat16),
        "query_weight": draw_query_weight(jax.random.fold_in(splits[13], 71), 0),
        "key_weight": draw_key_weight(jax.random.fold_in(splits[13], 71), 0),
        "value_weight": bell_draw(splits[6], (LAYERS, D, QW), D ** -0.5, 0.125, ((2, 8),)),
        "head_gain": jnp.clip(1.0 + 0.18 * jax.random.normal(splits[7], (LAYERS, QW), jnp.float32), 0.099609375, 1.8984375).astype(jnp.bfloat16),
        "out_weight": bell_draw(splits[8], (LAYERS, QW, D), QW ** -0.5, 0.1875, ((1, 8),)),
        "mlp_gain": jnp.clip(1.0 + 0.18 * jax.random.normal(splits[9], (D,), jnp.float32), 0.099609375, 1.8984375).astype(jnp.bfloat16),
        "gate_weight": bell_draw(splits[10], (D, FF), D ** -0.5, 0.125, ((1, 8),)),
        "up_weight": bell_draw(splits[11], (D, FF), D ** -0.5, 0.125, ((1, 8),)),
        "down_weight": bell_draw(splits[12], (FF, D), FF ** -0.5, 0.078125, ((0, 8),)),
    }


EPSILON = 1e-06

def row_scale(rows):
    return lax.rsqrt(lax.optimization_barrier(jnp.mean(rows * rows, axis=-1, keepdims=True)) + EPSILON)

def block_stats(queries, key_blocks, value_blocks):
    scores = jnp.einsum('the,bshe->bhts', queries.astype(jnp.float32), key_blocks.astype(jnp.float32), precision=lax.Precision.HIGHEST) * HEAD_DIM ** (-0.5)
    block_max = lax.optimization_barrier(jnp.max(scores, axis=-1))
    weights = jnp.exp(scores - block_max[..., None])
    block_total = lax.optimization_barrier(jnp.sum(weights, axis=-1))
    weights_low = lax.optimization_barrier(weights.astype(jnp.bfloat16))
    block_out = jnp.einsum('bhts,bshe->bthe', weights_low.astype(jnp.float32), value_blocks.astype(jnp.float32), precision=lax.Precision.HIGHEST).astype(jnp.bfloat16)
    return (jnp.swapaxes(block_max, 1, 2), jnp.swapaxes(block_total, 1, 2), block_out)

def merge_blocks(carry, stats):
    run_max, run_total, run_out = carry
    block_max, block_total, block_out = stats
    new_max = jnp.maximum(run_max, lax.optimization_barrier(jnp.max(block_max, axis=0)))
    keep = jnp.exp(run_max - new_max)
    factor = jnp.exp(block_max - new_max[None])
    total = run_total * keep + lax.optimization_barrier(jnp.sum(factor * block_total, axis=0))
    widened = lax.optimization_barrier(block_out).astype(jnp.float32)
    out = run_out * keep[..., None] + lax.optimization_barrier(jnp.sum(factor[..., None] * widened, axis=0))
    return (new_max, total, out)

def reference(source, target, source_gain, target_gain, query_weight, key_weight, value_weight, head_gain, out_weight, mlp_gain, gate_weight, up_weight, down_weight):
    src_wide = source.astype(jnp.float32)
    src_scale = row_scale(src_wide)
    state = target
    for layer in range(LAYERS):
        src_normed = (src_wide * src_scale * source_gain[layer].astype(jnp.float32)).astype(jnp.bfloat16)
        keys = jnp.dot(src_normed, key_weight[layer], preferred_element_type=jnp.float32).astype(jnp.bfloat16)
        values = jnp.dot(src_normed, value_weight[layer], preferred_element_type=jnp.float32).astype(jnp.bfloat16)
        keys = keys.reshape(N_SP, SRC_DEV, HEADS, HEAD_DIM)
        values = values.reshape(N_SP, SRC_DEV, HEADS, HEAD_DIM)
        state_wide = state.astype(jnp.float32)
        tgt_normed = (state_wide * row_scale(state_wide) * target_gain[layer].astype(jnp.float32)).astype(jnp.bfloat16)
        queries = jnp.dot(tgt_normed, query_weight[layer], preferred_element_type=jnp.float32).astype(jnp.bfloat16)
        queries = queries.reshape(TARGET, HEADS, HEAD_DIM)

        def advance(carry, pair):
            return (merge_blocks(carry, block_stats(queries, pair[0][None], pair[1][None])), None)
        start = (jnp.full((TARGET, HEADS), -jnp.inf, jnp.float32), jnp.zeros((TARGET, HEADS), jnp.float32), jnp.zeros((TARGET, HEADS, HEAD_DIM), jnp.float32))
        (run_max, run_total, run_out), _ = lax.scan(advance, start, (keys, values))
        attended = run_out / run_total[..., None]
        head_out = attended * row_scale(attended) * head_gain[layer].astype(jnp.float32).reshape(HEADS, HEAD_DIM)
        head_out = head_out.astype(jnp.bfloat16).reshape(TARGET, QW)
        projected = jnp.dot(head_out, out_weight[layer], preferred_element_type=jnp.float32)
        state = (state.astype(jnp.float32) + projected).astype(jnp.bfloat16)
    state_wide = state.astype(jnp.float32)
    mlp_in = (state_wide * row_scale(state_wide) * mlp_gain.astype(jnp.float32)).astype(jnp.bfloat16)
    gate = jnp.dot(mlp_in, gate_weight, preferred_element_type=jnp.float32)
    upward = jnp.dot(mlp_in, up_weight, preferred_element_type=jnp.float32)
    hidden = (jax.nn.silu(gate) * upward).astype(jnp.bfloat16)
    down = jnp.dot(hidden, down_weight, preferred_element_type=jnp.float32)
    return (state_wide + 0.5 * down).astype(jnp.bfloat16)
```

```python
import functools
import math

import jax
import jax.numpy as jnp
from jax import lax
from jax.experimental import pallas as pl
from jax.experimental.pallas import tpu as pltpu
from jax.sharding import PartitionSpec as P

HEAD_DIM = 128
EPSILON = 1e-06
NY = 4
MESH = pl.DeviceIdType.MESH
BF16 = jnp.bfloat16
F32 = jnp.float32


def rcopy(src, dst, send, recv, peer):
    return pltpu.make_async_remote_copy(
        src_ref=src,
        dst_ref=dst,
        send_sem=send,
        recv_sem=recv,
        device_id=peer,
        device_id_type=MESH,
    )


def at(index, size):
    return pl.ds(pl.multiple_of(index * size, size), size)


def body(
    nz,
    nx,
    source,
    target,
    source_gain,
    target_gain,
    query_weight,
    key_weight,
    value_weight,
    head_gain,
    out_weight,
    mlp_gain,
    gate_weight,
    up_weight,
    down_weight,
    out,
    src,
    tgt,
    wkv,
    wq,
    sgain,
    tgain,
    mgain,
    hgain,
    wo,
    wg,
    wu,
    wd,
    normed,
    kb,
    vb,
    qb,
    score,
    po,
    ps,
    pr,
    prs,
    ho,
    st,
    hid,
    part,
    pb,
    d2,
    comb,
    fr,
    lsem,
    ag_s,
    ag_r,
    wo_s,
    wo_r,
    k0_s,
    k0_r,
    k1_s,
    k1_r,
    q_s,
    q_r,
    p_s,
    p_r,
    rs_s,
    rs_r,
):
    ntp = 2 * nx
    depth = src.shape[1]
    src_rows = src.shape[0] // ntp
    own_rows = tgt.shape[0] // ntp
    rows = tgt.shape[0]
    block = src.shape[0]
    chunk = 2 * src_rows
    cols = depth // ntp
    hd = HEAD_DIM
    sp = lax.axis_index("sp")
    tp = lax.axis_index("tp")
    z = lax.div(sp, NY)
    y = lax.rem(sp, NY)
    x = lax.div(tp, 2)
    c = lax.rem(tp, 2)

    def device(zz, yy, xx, cc):
        return (zz * NY + yy, xx * 2 + cc)

    def x_peer(d):
        return device(z, y, lax.rem(x + d, nx), c)

    def y_peer(d):
        return device(z, lax.rem(y + d, NY), x, c)

    def z_peer(d):
        return device(lax.rem(z + d, nz), y, x, c)

    partner = device(z, y, x, 1 - c)
    x_order = (1, 3, 2) if nx == 4 else tuple(range(1, nx))

    loads = {}

    def load(name, index, source_ref, to):
        loads[name] = pltpu.make_async_copy(source_ref, to, lsem.at[index])
        loads[name].start()

    load("tgt", 0, target, tgt.at[at(tp, own_rows)])
    load("src", 1, source, src.at[at(tp, src_rows)])
    load("sgain", 2, source_gain, sgain)
    load("k", 3, key_weight, wkv.at[:, :, 0:hd])
    load("v", 4, value_weight, wkv.at[:, :, hd : 2 * hd])
    load("tgain", 5, target_gain, tgain)
    load("q", 6, query_weight, wq)
    load("hgain", 7, head_gain, hgain)
    load("mgain", 8, mlp_gain, mgain)
    load("wo", 9, out_weight.at[:, :, at(tp, cols)], wo.at[:, at(tp, hd)])
    load("wg", 10, gate_weight, wg)
    load("wu", 11, up_weight, wu)
    load("wd", 12, down_weight, wd)

    barrier = pltpu.get_barrier_semaphore()
    peers = [device(z, y, lax.rem(x + d // 2, nx), lax.rem(c + d, 2)) for d in range(1, ntp)]
    peers += [y_peer(d) for d in range(1, NY)]
    peers += [z_peer(d) for d in range(1, nz)]
    for peer in peers:
        pl.semaphore_signal(barrier, inc=1, device_id=peer, device_id_type=MESH)
    pl.semaphore_wait(barrier, len(peers))

    sent = []

    class Gather:
        def __init__(self, index, view):
            self.index = index
            self.view = view
            mine = view(tp)
            s, r = ag_s.at[index], ag_r.at[index]
            self.first = {d: rcopy(mine, mine, s.at[d], r.at[d], x_peer(d)) for d in x_order}
            self.own = rcopy(mine, mine, s.at[0], r.at[0], partner)
            self.passed = {}
            self.own.start()
            for d in x_order:
                self.first[d].start()
            sent.extend([self.own, *self.first.values()])

        def forward(self, d):
            self.first[d].wait_recv()
            owner = lax.rem(x + nx - d, nx) * 2 + c
            s, r = ag_s.at[self.index], ag_r.at[self.index]
            there = self.view(owner)
            self.passed[d] = rcopy(there, there, s.at[nx + d], r.at[nx + d], partner)
            self.passed[d].start()
            sent.append(self.passed[d])

        def finish(self):
            for d in x_order:
                self.forward(d)
            self.own.wait_recv()
            for d in x_order:
                self.passed[d].wait_recv()

    loads["tgt"].wait()
    gather_tgt = Gather(0, lambda j: tgt.at[at(j, own_rows)])
    loads["src"].wait()
    gather_src = Gather(1, lambda j: src.at[at(j, src_rows)])

    for layer in range(2):
        for d in range(1, ntp):
            to = device(z, y, lax.rem(x + d // 2, nx), lax.rem(c + d, 2))
            tp_to = to[1]
            cp = rcopy(
                out_weight.at[layer, :, at(tp_to, cols)],
                wo.at[layer, at(tp, hd)],
                wo_s.at[layer, d],
                wo_r.at[layer, d],
                to,
            )
            cp.start()
            sent.append(cp)

    def wait_wo(layer):
        for d in range(1, ntp):
            rcopy(
                out_weight.at[layer, :, at(tp, cols)],
                wo.at[layer, at(tp, hd)],
                wo_s.at[layer, d],
                wo_r.at[layer, d],
                partner,
            ).wait_recv()

    def norm_rows(from_ref, start, count, gain_ref, gain_row):
        step = 64

        def one(i, carry):
            at_from = pl.ds(pl.multiple_of(start + i * step, step), step)
            at_to = pl.ds(pl.multiple_of(i * step, step), step)
            total = jnp.zeros((step, 128), F32)
            for k in range(0, depth, 128):
                v = from_ref[at_from, k : k + 128].astype(F32)
                total += v * v
            mean = jnp.sum(total, axis=1, keepdims=True) * (1.0 / depth)
            scale = lax.rsqrt(mean + EPSILON)
            for k in range(0, depth, 128):
                v = from_ref[at_from, k : k + 128].astype(F32)
                g = gain_ref[gain_row : gain_row + 1, k : k + 128].astype(F32)
                normed[at_to, k : k + 128] = (v * scale * g).astype(BF16)
            return carry

        lax.fori_loop(0, count // step, one, 0)

    def project_source(layer, xx):
        norm_rows(src, xx * chunk, chunk, sgain, layer)
        kv = jnp.dot(normed[0:chunk], wkv[layer], preferred_element_type=F32)
        first = y * block + xx * chunk
        here = pl.ds(pl.multiple_of(first, chunk), chunk)
        kb[layer, here] = kv[:, 0:hd].astype(BF16)
        vb[layer, :, here] = jnp.transpose(kv[:, hd : 2 * hd]).astype(BF16)

    def k0_copies(xx, d):
        here = pl.ds(pl.multiple_of(y * block + xx * chunk, chunk), chunk)
        k = kb.at[0, here]
        v = vb.at[0, :, here]
        return (
            rcopy(k, k, k0_s.at[0, d, xx], k0_r.at[0, d, xx], y_peer(d)),
            rcopy(v, v, k0_s.at[1, d, xx], k0_r.at[1, d, xx], y_peer(d)),
        )

    def k1_copies(d):
        here = at(y, block)
        k = kb.at[1, here]
        v = vb.at[1, :, here]
        return (
            rcopy(k, k, k1_s.at[0, d], k1_r.at[0, d], y_peer(d)),
            rcopy(v, v, k1_s.at[1, d], k1_r.at[1, d], y_peer(d)),
        )

    def q_copy(layer, d):
        return rcopy(
            qb.at[layer, 0], qb.at[layer, d], q_s.at[layer, d], q_r.at[layer, d], z_peer(d)
        )

    def z_order(i):
        odd = lax.rem(i, 2)
        return odd * lax.div(i + 1, 2) + (1 - odd) * lax.rem(nz - lax.div(i, 2), nz)

    def project_query(layer, state_ref):
        norm_rows(state_ref, 0, rows, tgain, layer)
        q = jnp.dot(normed[0:rows], wq[layer], preferred_element_type=F32)
        qb[layer, 0] = q.astype(BF16)

        def send(i, carry):
            q_copy(layer, z_order(i)).start()
            return carry

        lax.fori_loop(1, nz, send, 0)

    def send_k0(xx):
        for d in (1, 3, 2):
            for cp in k0_copies(xx, d):
                cp.start()

    loads["sgain"].wait()
    loads["k"].wait()
    loads["v"].wait()
    gather_src.own.wait_recv()
    project_source(0, x)
    send_k0(x)
    gather_tgt.finish()
    loads["tgain"].wait()
    loads["q"].wait()
    project_query(0, tgt)
    for d in x_order:
        gather_src.forward(d)
    for d in x_order:
        gather_src.passed[d].wait_recv()
        xx = lax.rem(x + nx - d, nx)
        project_source(0, xx)
        send_k0(xx)

    def project_one(i, carry):
        project_source(1, i)
        return carry

    lax.fori_loop(0, nx, project_one, 0)
    for d in (1, 3, 2):
        for cp in k1_copies(d):
            cp.start()

    factor = math.log2(math.e) * hd**-0.5

    def p_copies(layer, d):
        return (
            rcopy(po.at[layer, d], pr.at[layer, d], p_s.at[layer, 0, d], p_r.at[layer, 0, d], z_peer(nz - d)),
            rcopy(ps.at[layer, d], prs.at[layer, d], p_s.at[layer, 1, d], p_r.at[layer, 1, d], z_peer(nz - d)),
        )

    def attend(layer):
        def one(i, carry):
            d = z_order(i)

            @pl.when(i > 0)
            def _():
                q_copy(layer, d).wait_recv()

            q = qb[layer, d]
            top = None
            for b in range(NY):
                here = slice(b * block, (b + 1) * block)
                s = lax.dot_general(
                    kb[layer, here], q, (((1,), (1,)), ((), ())), preferred_element_type=F32
                )
                score[here] = s
                m = jnp.max(s, axis=0, keepdims=True)
                top = m if top is None else jnp.maximum(top, m)
            shift = top * factor
            total = jnp.zeros((1, rows), F32)
            acc = jnp.zeros((hd, rows), F32)
            for b in range(NY):
                here = slice(b * block, (b + 1) * block)
                w = jnp.exp2(score[here] * factor - shift)
                total += jnp.sum(w, axis=0, keepdims=True)
                acc += jnp.dot(vb[layer, :, here], w.astype(BF16), preferred_element_type=F32)
            low = acc.astype(BF16)
            which = lax.broadcasted_iota(jnp.int32, (8, rows), 0)
            stats = jnp.where(which == 0, top, total)

            @pl.when(i == 0)
            def _():
                pr[layer, 0] = low
                prs[layer, 0] = stats

            @pl.when(i > 0)
            def _():
                po[layer, d] = low
                ps[layer, d] = stats
                for cp in p_copies(layer, d):
                    cp.start()

            return carry

        lax.fori_loop(0, nz, one, 0)

    def merge(layer):
        def wait(d, carry):
            for cp in p_copies(layer, d):
                cp.wait_recv()
            return carry

        lax.fori_loop(1, nz, wait, 0)
        top = prs[layer, 0, 0:1]
        for d in range(1, nz):
            top = jnp.maximum(top, prs[layer, d, 0:1])
        total = jnp.zeros((1, rows), F32)
        acc = jnp.zeros((hd, rows), F32)
        for d in range(nz):
            f = jnp.exp2((prs[layer, d, 0:1] - top) * factor)
            total += f * prs[layer, d, 1:2]
            acc += f * pr[layer, d].astype(F32)
        attended = acc / total
        mean = jnp.mean(attended * attended, axis=0, keepdims=True)
        scaled = jnp.transpose(attended * lax.rsqrt(mean + EPSILON))
        gain = hgain[layer : layer + 1, :].astype(F32)
        ho[layer, :, at(tp, hd)] = (scaled * gain).astype(BF16)

    def advance(layer, old_ref):
        Gather(2 + 2 * layer, lambda j: ho.at[layer, :, at(j, hd)]).finish()
        wait_wo(layer)
        add = jnp.dot(ho[layer], wo[layer], preferred_element_type=F32)
        new = old_ref[:, at(tp, cols)].astype(F32) + add
        st[layer, :, at(tp, cols)] = new.astype(BF16)
        Gather(3 + 2 * layer, lambda j: st.at[layer, :, at(j, cols)]).finish()

    for d in range(1, NY):
        for xx in range(nx):
            for cp in k0_copies(xx, d):
                cp.wait_recv()
    attend(0)
    loads["hgain"].wait()
    loads["wo"].wait()
    merge(0)
    advance(0, tgt)
    project_query(1, st.at[0])
    for d in range(1, NY):
        for cp in k1_copies(d):
            cp.wait_recv()
    attend(1)
    merge(1)
    advance(1, st.at[0])

    loads["mgain"].wait()
    loads["wg"].wait()
    loads["wu"].wait()
    loads["wd"].wait()
    norm_rows(st.at[1], 0, rows, mgain, 0)
    over = (((1,), (1,)), ((), ()))
    gate = lax.dot_general(wg[...], normed[0:rows], over, preferred_element_type=F32)
    up = lax.dot_general(wu[...], normed[0:rows], over, preferred_element_type=F32)
    hid[...] = jnp.transpose(gate / (1.0 + jnp.exp(-gate)) * up).astype(BF16)
    pieces = 2
    width = depth // pieces

    def d2_copy(n):
        w = slice(n * width, (n + 1) * width)
        return rcopy(pb.at[:, :, w], d2.at[:, :, w], rs_s.at[n, 0], rs_r.at[n, 0], partner)

    def fr_copy(n, d):
        w = slice(n * width, (n + 1) * width)
        return rcopy(comb.at[d, :, w], fr.at[d, :, w], rs_s.at[n, d], rs_r.at[n, d], x_peer(d))

    for n in range(pieces):
        w = slice(n * width, (n + 1) * width)
        down = jnp.dot(hid[...], wd[:, w], preferred_element_type=F32)
        part[:, :, :, w] = down.reshape(nx, 2, own_rows, width)
        pb[:, :, w] = part[:, 1 - c, :, w].astype(BF16)
        d2_copy(n).start()
    for n in range(pieces):
        w = slice(n * width, (n + 1) * width)
        d2_copy(n).wait_recv()
        for d in x_order:
            xx = lax.rem(x + d, nx)
            comb[d, :, w] = (part[xx, c, :, w] + d2[xx, :, w].astype(F32)).astype(BF16)
            fr_copy(n, d).start()
    for n in range(pieces):
        w = slice(n * width, (n + 1) * width)
        down = part[x, c, :, w] + d2[x, :, w].astype(F32)
        for d in x_order:
            fr_copy(n, d).wait_recv()
            down += fr[d, :, w].astype(F32)
        state = st[1, at(tp, own_rows), w].astype(F32)
        out[:, w] = (state + 0.5 * down).astype(BF16)

    for cp in sent:
        cp.wait_send()
    for d in range(1, NY):
        for xx in range(nx):
            for cp in k0_copies(xx, d):
                cp.wait_send()
        for cp in k1_copies(d):
            cp.wait_send()
    for layer in range(2):
        for d in range(1, nz):
            q_copy(layer, d).wait_send()
            for cp in p_copies(layer, d):
                cp.wait_send()
    for n in range(pieces):
        d2_copy(n).wait_send()
        for d in x_order:
            fr_copy(n, d).wait_send()


def local(nz, nx, *args):
    source, target = args[0], args[1]
    ntp = 2 * nx
    depth = source.shape[1]
    block = source.shape[0] * ntp
    rows = target.shape[0] * ntp
    own = target.shape[0]
    ffl = args[10].shape[1]
    hd = HEAD_DIM
    args = list(args)
    args[9] = args[9].reshape(1, depth)
    args[10] = args[10].T
    args[11] = args[11].T
    vmem = pltpu.VMEM
    dma = pltpu.SemaphoreType.DMA
    scratch = [
        vmem((block, depth), BF16),
        vmem((rows, depth), BF16),
        vmem((2, depth, 2 * hd), BF16),
        vmem((2, depth, hd), BF16),
        vmem((2, depth), BF16),
        vmem((2, depth), BF16),
        vmem((1, depth), BF16),
        vmem((2, hd), BF16),
        vmem((2, ntp * hd, depth // ntp), BF16),
        vmem((ffl, depth), BF16),
        vmem((ffl, depth), BF16),
        vmem((ffl, depth), BF16),
        vmem((rows, depth), BF16),
        vmem((2, NY * block, hd), BF16),
        vmem((2, hd, NY * block), BF16),
        vmem((2, nz, rows, hd), BF16),
        vmem((NY * block, rows), F32),
        vmem((2, nz, hd, rows), BF16),
        vmem((2, nz, 8, rows), F32),
        vmem((2, nz, hd, rows), BF16),
        vmem((2, nz, 8, rows), F32),
        vmem((2, rows, ntp * hd), BF16),
        vmem((2, rows, depth), BF16),
        vmem((rows, ffl), BF16),
        vmem((nx, 2, own, depth), F32),
        vmem((nx, own, depth), BF16),
        vmem((nx, own, depth), BF16),
        vmem((nx, own, depth), BF16),
        vmem((nx, own, depth), BF16),
        dma((13,)),
        dma((6, 2 * nx)),
        dma((6, 2 * nx)),
        dma((2, ntp)),
        dma((2, ntp)),
        dma((2, NY, nx)),
        dma((2, NY, nx)),
        dma((2, NY)),
        dma((2, NY)),
        dma((2, nz)),
        dma((2, nz)),
        dma((2, 2, nz)),
        dma((2, 2, nz)),
        dma((2, nx)),
        dma((2, nx)),
    ]
    return pl.pallas_call(
        functools.partial(body, nz, nx),
        name="decoder",
        out_shape=jax.ShapeDtypeStruct(target.shape, BF16),
        in_specs=[pl.BlockSpec(memory_space=pl.ANY)] * len(args),
        out_specs=pl.BlockSpec(memory_space=pltpu.VMEM),
        scratch_shapes=scratch,
        compiler_params=pltpu.CompilerParams(
            collective_id=0, has_side_effects=True, vmem_limit_bytes=60 * 1024 * 1024
        ),
    )(*args)


def solution(mesh):
    nz = mesh.shape["sp"] // NY
    nx = mesh.shape["tp"] // 2
    in_specs = (
        P(("sp", "tp"), None),
        P(("sp", "tp"), None),
        P(),
        P(),
        P(None, None, "tp"),
        P(None, None, "tp"),
        P(None, None, "tp"),
        P(None, "tp"),
        P(None, "tp", None),
        P(),
        P(None, "tp"),
        P(None, "tp"),
        P("tp", None),
    )
    out_specs = P(("sp", "tp"), None)
    return jax.shard_map(
        functools.partial(local, nz, nx),
        mesh=mesh,
        in_specs=in_specs,
        out_specs=out_specs,
        check_vma=False,
    )
```

```python
import functools
import math

import jax
import jax.numpy as jnp
from jax import lax
from jax.experimental import pallas as pl
from jax.experimental.pallas import tpu as pltpu
from jax.sharding import PartitionSpec as P

HEAD_DIM = 128
EPSILON = 1e-06
NY = 4
MESH = pl.DeviceIdType.MESH
BF16 = jnp.bfloat16
F32 = jnp.float32


def rcopy(src, dst, send, recv, peer):
    return pltpu.make_async_remote_copy(
        src_ref=src,
        dst_ref=dst,
        send_sem=send,
        recv_sem=recv,
        device_id=peer,
        device_id_type=MESH,
    )


def at(index, size):
    return pl.ds(pl.multiple_of(index * size, size), size)


def body(
    nz,
    nx,
    source,
    target,
    source_gain,
    target_gain,
    query_weight,
    key_weight,
    value_weight,
    head_gain,
    out_weight,
    mlp_gain,
    gate_weight,
    up_weight,
    down_weight,
    out,
    src,
    tgt,
    wkv,
    wq,
    sgain,
    tgain,
    mgain,
    hgain,
    wo,
    wo1,
    wg,
    wu,
    wd,
    normed,
    kb,
    vb,
    qb,
    score,
    po,
    ps,
    pr,
    prs,
    ho,
    st,
    hid,
    part,
    pb,
    d2,
    comb,
    fr,
    mixed,
    lsem,
    src_s,
    src_r,
    ag_s,
    ag_r,
    wo_s,
    wo_r,
    k_s,
    k_r,
    q_s,
    q0_r,
    q_r,
    p_s,
    p_r,
    d_s,
    d_r,
    f_s,
    f_r,
    o_s,
):
    ntp = 2 * nx
    depth = src.shape[1]
    src_rows = src.shape[0] // ntp
    own_rows = tgt.shape[0] // ntp
    rows = tgt.shape[0]
    block = src.shape[0]
    chunk = 2 * src_rows
    cols = depth // ntp
    hd = HEAD_DIM
    sp = lax.axis_index("sp")
    tp = lax.axis_index("tp")
    z = lax.div(sp, NY)
    y = lax.rem(sp, NY)
    x = lax.div(tp, 2)
    c = lax.rem(tp, 2)

    def device(zz, yy, xx, cc):
        return (zz * NY + yy, xx * 2 + cc)

    def x_peer(d):
        return device(z, y, lax.rem(x + d, nx), c)

    def y_peer(d):
        return device(z, lax.rem(y + d, NY), x, c)

    def z_peer(d):
        return device(lax.rem(z + d, nz), y, x, c)

    partner = device(z, y, x, 1 - c)
    x_order = (1, 3, 2) if nx == 4 else tuple(range(1, nx))

    loads = {}

    def load(name, index, source_ref, to):
        loads[name] = pltpu.make_async_copy(source_ref, to, lsem.at[index])
        loads[name].start()

    load("tgt", 0, target, tgt.at[at(tp, own_rows)])
    load("src", 1, source, src.at[at(tp, src_rows)])
    load("sgain", 2, source_gain, sgain)
    load("k", 3, key_weight, wkv.at[:, :, 0:hd])
    load("v", 4, value_weight, wkv.at[:, :, hd : 2 * hd])
    load("tgain", 5, target_gain, tgain)
    load("q", 6, query_weight, wq)
    load("hgain", 7, head_gain, hgain)
    load("mgain", 8, mlp_gain, mgain)
    load("wo", 9, out_weight.at[0, :, at(tp, cols)], wo.at[at(tp, hd)])
    load("wo1", 13, out_weight.at[1], wo1.at[at(tp, hd)])
    load("wg", 10, gate_weight, wg)
    load("wu", 11, up_weight, wu)
    load("wd", 12, down_weight, wd)

    scope = jax.named_scope
    barrier = pltpu.get_barrier_semaphore()
    peers = [device(z, y, lax.rem(x + d // 2, nx), lax.rem(c + d, 2)) for d in range(1, ntp)]
    peers += [y_peer(d) for d in range(1, NY)]
    peers += [z_peer(d) for d in range(1, nz)]
    with scope("barrier"):
        for peer in peers:
            pl.semaphore_signal(barrier, inc=1, device_id=peer, device_id_type=MESH)
        pl.semaphore_wait(barrier, len(peers))

    def all_sent(ref, sem):
        rcopy(ref, ref, sem, sem, partner).wait_send()

    def all_here(ref, sem):
        rcopy(ref, ref, sem, sem, partner).wait_recv()

    class Gather:
        def __init__(self, index, view):
            self.view = view
            self.send = ag_s.at[index]
            self.near = ag_r.at[index, 0]
            mine = view(tp)
            self.first = {d: rcopy(mine, mine, self.send, ag_r.at[index, d], x_peer(d)) for d in x_order}
            rcopy(mine, mine, self.send, self.near, partner).start()
            for d in x_order:
                self.first[d].start()

        def forward(self):
            for d in x_order:
                self.first[d].wait_recv()
                there = self.view(lax.rem(x + nx - d, nx) * 2 + c)
                rcopy(there, there, self.send, self.near, partner).start()

        def finish(self, near_bytes, sent_bytes):
            all_here(near_bytes, self.near)
            all_sent(sent_bytes, self.send)

    loads["src"].wait()

    half = src_rows // 2
    left, right = x_peer(nx - 1), x_peer(1)
    tp_left = lax.rem(x + nx - 1, nx) * 2 + c
    tp_right = lax.rem(x + 1, nx) * 2 + c
    tp_far = lax.rem(x + 2, nx) * 2 + c

    def src_copy(index, owner, first, count, to):
        ref = src.at[pl.ds(pl.multiple_of(owner * src_rows + first, half), count)]
        rcopy(ref, ref, src_s, src_r.at[index], to).start()

    def src_wait(index, count):
        ref = src.at[pl.ds(0, count)]
        all_here(ref, src_r.at[index])

    src_copy(0, tp, 0, src_rows, partner)
    src_copy(1, tp, 0, half, right)
    src_copy(2, tp, half, half, left)
    src_copy(3, tp, half, half, right)
    src_copy(4, tp, 0, half, left)
    loads["tgt"].wait()
    gather_tgt = Gather(0, lambda j: tgt.at[at(j, own_rows)])

    def out_copy(d):
        to = device(z, y, lax.rem(x + d // 2, nx), lax.rem(c + d, 2))
        return rcopy(
            out_weight.at[0, :, at(to[1], cols)], wo.at[at(tp, hd)], wo_s, wo_r, to
        )

    factor = math.log2(math.e) * hd**-0.5

    def norm_rows(from_ref, start, count, gain_of):
        step = 64

        def one(i, carry):
            at_from = pl.ds(pl.multiple_of(start + i * step, step), step)
            at_to = pl.ds(pl.multiple_of(i * step, step), step)
            total = jnp.zeros((step, 128), F32)
            for k in range(0, depth, 128):
                v = from_ref[at_from, k : k + 128].astype(F32)
                total += v * v
            mean = jnp.sum(total, axis=1, keepdims=True) * (1.0 / depth)
            scale = lax.rsqrt(mean + EPSILON)
            for k in range(0, depth, 128):
                v = from_ref[at_from, k : k + 128].astype(F32)
                g = gain_of(k).astype(F32)
                normed[at_to, k : k + 128] = (v * scale * g).astype(BF16)
            return carry

        lax.fori_loop(0, count // step, one, 0)

    def project_source(layer, xx):
        norm_rows(src, xx * chunk, chunk, lambda k: sgain[layer : layer + 1, k : k + 128])
        kv = jnp.dot(normed[0:chunk], wkv[layer], preferred_element_type=F32)
        first = y * block + xx * chunk
        here = pl.ds(pl.multiple_of(first, chunk), chunk)
        kb[layer, here] = kv[:, 0:hd].astype(BF16)
        vb[layer, :, here] = jnp.transpose(kv[:, hd : 2 * hd]).astype(BF16)

    def k0_copies(xx, d):
        here = pl.ds(pl.multiple_of(y * block + xx * chunk, chunk), chunk)
        k = kb.at[0, here]
        v = vb.at[0, :, here]
        return (
            rcopy(k, k, k_s.at[0, 0], k_r.at[0, 0], y_peer(d)),
            rcopy(v, v, k_s.at[0, 1], k_r.at[0, 1], y_peer(d)),
        )

    def k1_copies(d):
        here = at(y, block)
        k = kb.at[1, here]
        v = vb.at[1, :, here]
        return (
            rcopy(k, k, k_s.at[1, 0], k_r.at[1, 0], y_peer(d)),
            rcopy(v, v, k_s.at[1, 1], k_r.at[1, 1], y_peer(d)),
        )

    def z_order(i):
        odd = lax.rem(i, 2)
        return odd * lax.div(i + 1, 2) + (1 - odd) * lax.rem(nz - lax.div(i, 2), nz)

    def q_copy(layer, slot, source_slot=0, d=None):
        to = z_peer(z_order(slot) if d is None else d)
        return rcopy(
            qb.at[layer, source_slot],
            qb.at[layer, slot],
            q_s.at[layer],
            q0_r if layer == 0 else q_r.at[slot],
            to,
        )

    def project_query(layer, state_ref):
        norm_rows(state_ref, 0, rows, lambda k: tgain[layer : layer + 1, k : k + 128])
        q = jnp.dot(normed[0:rows], wq[layer], preferred_element_type=F32)
        qb[layer, 0] = (q * factor).astype(BF16)

        def send(i, carry):
            q_copy(layer, i).start()
            return carry

        lax.fori_loop(1, nz if layer == 0 else 5, send, 0)

    def send_k0(xx):
        for d in (1, 3, 2):
            for cp in k0_copies(xx, d):
                cp.start()

    with scope("wait_own"):
        loads["sgain"].wait()
        loads["k"].wait()
        loads["v"].wait()
        src_wait(0, src_rows)
    with scope("kv_own"):
        project_source(0, x)
        send_k0(x)
    with scope("wait_src"):
        src_wait(1, half)
        src_copy(5, tp_left, 0, half, right)
        src_wait(2, half)
        src_copy(6, tp_right, half, half, left)
        src_wait(3, half)
        src_copy(7, tp_left, 0, src_rows, partner)
        src_wait(4, half)
        src_copy(8, tp_right, 0, src_rows, partner)
        src_wait(7, src_rows)
    for d in range(1, ntp):
        out_copy(d).start()
    with scope("kv_left"):
        xx = lax.rem(x + nx - 1, nx)
        project_source(0, xx)
        send_k0(xx)
    src_wait(8, src_rows)
    with scope("kv_right"):
        xx = lax.rem(x + 1, nx)
        project_source(0, xx)
        send_k0(xx)
    with scope("wait_tgt"):
        gather_tgt.forward()
        gather_tgt.finish(tgt.at[0 : 4 * own_rows], tgt.at[0 : 7 * own_rows])
        loads["tgain"].wait()
        loads["q"].wait()
    with scope("q0"):
        project_query(0, tgt)
    with scope("wait_far"):
        src_wait(5, half)
        src_copy(9, tp_far, 0, half, partner)
        src_wait(6, half)
        src_copy(10, tp_far, half, half, partner)
        src_wait(9, half)
        src_wait(10, half)
    with scope("kv_far"):
        xx = lax.rem(x + 2, nx)
        project_source(0, xx)
        send_k0(xx)
    loads["wo1"].wait()
    first_rows = 80

    def wo1_first(j):
        return wo1.at[pl.ds(pl.multiple_of(j * hd, hd), first_rows)]

    def wo1_rest(j):
        return wo1.at[pl.ds(pl.multiple_of(j * hd + first_rows, 16), hd - first_rows)]

    gather_wo1 = Gather(3, wo1_first)

    def project_one(i, carry):
        project_source(1, i)
        return carry

    with scope("kv1"):
        lax.fori_loop(0, nx, project_one, 0)
        for d in (1, 3, 2):
            for cp in k1_copies(d):
                cp.start()

    def p_copies(layer, slot):
        to = z_peer(nz - z_order(slot))
        return (
            rcopy(
                po.at[layer, slot], pr.at[layer, slot], p_s.at[layer, 0], p_r.at[layer, 0], to
            ),
            rcopy(
                ps.at[layer, slot], prs.at[layer, slot], p_s.at[layer, 1], p_r.at[layer, 1], to
            ),
        )

    def attend(layer, first, count):
        wide = count * rows
        q = qb[layer, pl.ds(first, count)].reshape(wide, hd)
        top = None
        for b in range(NY):
            here = slice(b * block, (b + 1) * block)
            s = lax.dot_general(
                kb[layer, here], q, (((1,), (1,)), ((), ())), preferred_element_type=F32
            )
            score[here, 0:wide] = s
            m = jnp.max(s, axis=0, keepdims=True)
            top = m if top is None else jnp.maximum(top, m)
        total = jnp.zeros((1, wide), F32)
        acc = jnp.zeros((hd, wide), F32)
        for b in range(NY):
            here = slice(b * block, (b + 1) * block)
            w = jnp.exp2(score[here, 0:wide] - top)
            total += jnp.sum(w, axis=0, keepdims=True)
            acc += jnp.dot(vb[layer, :, here], w.astype(BF16), preferred_element_type=F32)
        low = acc.astype(BF16)
        which = lax.broadcasted_iota(jnp.int32, (8, wide), 0)
        stats = jnp.where(which == 0, top, total)
        for j in range(count):
            to_out, to_stats = (pr, prs) if isinstance(first, int) and first == 0 else (po, ps)
            to_out[layer, first + j] = low[:, j * rows : (j + 1) * rows]
            to_stats[layer, first + j] = stats[:, j * rows : (j + 1) * rows]
            if to_out is po:
                for cp in p_copies(layer, first + j):
                    cp.start()

    def q_wait(layer, slot):
        q_copy(layer, slot).wait_recv()

    def attend_first():
        all_here(qb.at[0, 1:nz], q0_r)
        attend(0, nz - 1, 1)

        def pair(i, carry):
            attend(0, nz - 3 - 2 * i, 2)
            return carry

        lax.fori_loop(0, (nz - 2) // 2, pair, 0)
        attend(0, 0, 1)

    def relays():
        return (
            q_copy(1, 5, 3, 1),
            q_copy(1, 6, 4, nz - 1),
            q_copy(1, 7, 3 + c, 2 + c * (nz - 4)),
        )

    def attend_second():
        attend(1, 0, 1)

        def pair(i, carry):
            first = 1 + 2 * i
            with scope("wait_q"):
                q_wait(1, first)
                q_wait(1, first + 1)

            @pl.when(i == 1)
            def _():
                for cp in relays():
                    cp.start()

            attend(1, first, 2)
            return carry

        lax.fori_loop(0, (nz - 2) // 2, pair, 0)
        with scope("wait_q"):
            q_wait(1, nz - 1)
        attend(1, nz - 1, 1)

    def merge(layer):
        with scope("wait_p"):
            all_here(pr.at[layer, 1:nz], p_r.at[layer, 0])
            all_here(prs.at[layer, 1:nz], p_r.at[layer, 1])
        top = prs[layer, 0, 0:1]
        for d in range(1, nz):
            top = jnp.maximum(top, prs[layer, d, 0:1])
        total = jnp.zeros((1, rows), F32)
        acc = jnp.zeros((hd, rows), F32)
        for d in range(nz):
            f = jnp.exp2(prs[layer, d, 0:1] - top)
            total += f * prs[layer, d, 1:2]
            acc += f * pr[layer, d].astype(F32)
        attended = acc / total
        mean = jnp.mean(attended * attended, axis=0, keepdims=True)
        scaled = jnp.transpose(attended * lax.rsqrt(mean + EPSILON))
        gain = hgain[layer : layer + 1, :].astype(F32)
        ho[layer, :, at(tp, hd)] = (scaled * gain).astype(BF16)

    def gather_heads(layer):
        with scope("gather_ho"):
            gather = Gather(1 if layer == 0 else 5, lambda j: ho.at[layer, :, at(j, hd)])
            gather.forward()
            gather.finish(ho.at[layer, :, 0 : 4 * hd], ho.at[layer, :, 0 : 7 * hd])

    def kv_wait(layer):
        most = (NY - 1) * block
        all_here(kb.at[layer, 0:most], k_r.at[layer, 0])
        all_here(vb.at[layer, :, 0:most], k_r.at[layer, 1])

    with scope("wait_kv0"):
        kv_wait(0)
    with scope("attend0"):
        attend_first()
    loads["hgain"].wait()
    loads["wo"].wait()
    with scope("merge0"):
        merge(0)
    gather_heads(0)
    with scope("wait_wo"):
        all_here(wo.at[0 : (ntp - 1) * hd], wo_r)
    add = jnp.dot(ho[0], wo[...], preferred_element_type=F32)
    new = tgt[:, at(tp, cols)].astype(F32) + add
    st[0, :, at(tp, cols)] = new.astype(BF16)
    with scope("gather_st"):
        gather_st = Gather(2, lambda j: st.at[0, :, at(j, cols)])
        gather_wo1.forward()
        gather_st.forward()
        gather_st.finish(st.at[0, :, 0 : 4 * cols], st.at[0, :, 0 : 7 * cols])
    with scope("wo1"):
        gather_wo1.finish(wo1.at[0 : 4 * first_rows], wo1.at[0 : 7 * first_rows])
        gather_wo1 = Gather(4, wo1_rest)
    with scope("q1"):
        project_query(1, st.at[0])
    with scope("wait_kv1"):
        kv_wait(1)
    with scope("attend1"):
        attend_second()
    with scope("wo1_rest"):
        gather_wo1.forward()
    with scope("merge1"):
        merge(1)
    gather_heads(1)
    with scope("wo1_wait"):
        gather_wo1.finish(
            wo1.at[0 : 4 * (hd - first_rows)], wo1.at[0 : 7 * (hd - first_rows)]
        )
    with scope("out1"):

        def out_piece(i, carry):
            w = at(i, 512)
            add = jnp.dot(ho[1], wo1[:, w], preferred_element_type=F32)
            st[1, :, w] = (st[0, :, w].astype(F32) + add).astype(BF16)
            return carry

        lax.fori_loop(0, depth // 512, out_piece, 0)

    loads["mgain"].wait()
    loads["wg"].wait()
    loads["wu"].wait()
    loads["wd"].wait()
    with scope("mlp_norm"):
        norm_rows(st.at[1], 0, rows, lambda k: mgain[k // 128 : k // 128 + 1, :])
    over = (((1,), (1,)), ((), ()))
    with scope("gate"):
        gate = lax.dot_general(wg[...], normed[0:rows], over, preferred_element_type=F32)
        up = lax.dot_general(wu[...], normed[0:rows], over, preferred_element_type=F32)
        hid[...] = jnp.transpose(gate / (1.0 + jnp.exp(-gate)) * up).astype(BF16)
    pieces = 4
    width = depth // pieces

    def d2_copy(n):
        w = slice(n * width, (n + 1) * width)
        return rcopy(pb.at[:, :, w], d2.at[:, :, w], d_s, d_r.at[n], partner)

    def fr_copy(n, d):
        w = slice(n * width, (n + 1) * width)
        return rcopy(comb.at[d, :, w], fr.at[d, :, w], f_s, f_r.at[n], x_peer(d))

    def pair_sum(n):
        w = slice(n * width, (n + 1) * width)
        with scope("wait_d2"):
            d2_copy(n).wait_recv()
        for d in x_order:
            xx = lax.rem(x + d, nx)
            comb[d, :, w] = (part[xx, c, :, w] + d2[xx, :, w].astype(F32)).astype(BF16)
            fr_copy(n, d).start()

    for n in range(pieces):
        w = slice(n * width, (n + 1) * width)
        with scope("down"):
            down = jnp.dot(hid[...], wd[:, w], preferred_element_type=F32)
            part[:, :, :, w] = down.reshape(nx, 2, own_rows, width)
            pb[:, :, w] = part[:, 1 - c, :, w].astype(BF16)
            d2_copy(n).start()
        if n > 0:
            pair_sum(n - 1)
    pair_sum(pieces - 1)
    def out_piece_copy(n):
        w = slice(n * width, (n + 1) * width)
        return pltpu.make_async_copy(mixed.at[:, w], out.at[:, w], o_s.at[n])

    for n in range(pieces):
        w = slice(n * width, (n + 1) * width)
        down = part[x, c, :, w] + d2[x, :, w].astype(F32)
        with scope("wait_fr"):
            all_here(fr.at[1:nx, :, w], f_r.at[n])
        for d in x_order:
            down += fr[d, :, w].astype(F32)
        state = st[1, at(tp, own_rows), w].astype(F32)
        mixed[:, w] = (state + 0.5 * down).astype(BF16)
        out_piece_copy(n).start()

    with scope("drain"):
        all_sent(src.at[0 : 7 * src_rows], src_s)
        all_sent(wo.at[0 : (ntp - 1) * hd], wo_s)
        for layer in range(2):
            all_sent(kb.at[layer, 0 : (NY - 1) * block], k_s.at[layer, 0])
            all_sent(vb.at[layer, :, 0 : (NY - 1) * block], k_s.at[layer, 1])
            all_sent(qb.at[layer, 1:nz], q_s.at[layer])
            all_sent(po.at[layer, 1:nz], p_s.at[layer, 0])
            all_sent(ps.at[layer, 1:nz], p_s.at[layer, 1])
        all_sent(pb, d_s)
        all_sent(comb.at[1:nx], f_s)
        for n in range(pieces):
            out_piece_copy(n).wait()


def local(nz, nx, *args):
    source, target = args[0], args[1]
    ntp = 2 * nx
    depth = source.shape[1]
    block = source.shape[0] * ntp
    rows = target.shape[0] * ntp
    own = target.shape[0]
    ffl = args[10].shape[1]
    hd = HEAD_DIM
    args = list(args)
    args[9] = args[9].reshape(depth // 128, 128)
    args[10] = args[10].T
    args[11] = args[11].T
    vmem = pltpu.VMEM
    dma = pltpu.SemaphoreType.DMA
    scratch = [
        vmem((block, depth), BF16),
        vmem((rows, depth), BF16),
        vmem((2, depth, 2 * hd), BF16),
        vmem((2, depth, hd), BF16),
        vmem((2, depth), BF16),
        vmem((2, depth), BF16),
        vmem((depth // 128, 128), BF16),
        vmem((2, hd), BF16),
        vmem((ntp * hd, depth // ntp), BF16),
        vmem((ntp * hd, depth), BF16),
        vmem((ffl, depth), BF16),
        vmem((ffl, depth), BF16),
        vmem((ffl, depth), BF16),
        vmem((rows, depth), BF16),
        vmem((2, NY * block, hd), BF16),
        vmem((2, hd, NY * block), BF16),
        vmem((2, nz, rows, hd), BF16),
        vmem((NY * block, 2 * rows), F32),
        vmem((2, nz, hd, rows), BF16),
        vmem((2, nz, 8, rows), F32),
        vmem((2, nz, hd, rows), BF16),
        vmem((2, nz, 8, rows), F32),
        vmem((2, rows, ntp * hd), BF16),
        vmem((2, rows, depth), BF16),
        vmem((rows, ffl), BF16),
        vmem((nx, 2, own, depth), F32),
        vmem((nx, own, depth), BF16),
        vmem((nx, own, depth), BF16),
        vmem((nx, own, depth), BF16),
        vmem((nx, own, depth), BF16),
        vmem((own, depth), BF16),
        dma((14,)),
        dma(()),
        dma((11,)),
        dma((6,)),
        dma((6, nx)),
        dma(()),
        dma(()),
        dma((2, 2)),
        dma((2, 2)),
        dma((2,)),
        dma(()),
        dma((nz,)),
        dma((2, 2)),
        dma((2, 2)),
        dma(()),
        dma((4,)),
        dma(()),
        dma((4,)),
        dma((4,)),
    ]
    return pl.pallas_call(
        functools.partial(body, nz, nx),
        name="decoder",
        out_shape=jax.ShapeDtypeStruct(target.shape, BF16),
        in_specs=[pl.BlockSpec(memory_space=pl.ANY)] * len(args),
        out_specs=pl.BlockSpec(memory_space=pl.ANY),
        scratch_shapes=scratch,
        compiler_params=pltpu.CompilerParams(
            collective_id=0, has_side_effects=True, vmem_limit_bytes=60 * 1024 * 1024
        ),
    )(*args)


def solution(mesh):
    nz = mesh.shape["sp"] // NY
    nx = mesh.shape["tp"] // 2
    in_specs = (
        P(("sp", "tp"), None),
        P(("sp", "tp"), None),
        P(),
        P(),
        P(None, None, "tp"),
        P(None, None, "tp"),
        P(None, None, "tp"),
        P(None, "tp"),
        P(None, "tp", None),
        P(),
        P(None, "tp"),
        P(None, "tp"),
        P("tp", None),
    )
    out_specs = P(("sp", "tp"), None)
    return jax.shard_map(
        functools.partial(local, nz, nx),
        mesh=mesh,
        in_specs=in_specs,
        out_specs=out_specs,
        check_vma=False,
    )
```

```python
import functools
import math

import jax
import jax.numpy as jnp
from jax import lax
from jax.experimental import pallas as pl
from jax.experimental.pallas import tpu as pltpu
from jax.sharding import PartitionSpec as P

HEAD_DIM = 128
EPSILON = 1e-06
NY = 4
MESH = pl.DeviceIdType.MESH
BF16 = jnp.bfloat16
F32 = jnp.float32


def rcopy(src, dst, send, recv, peer):
    return pltpu.make_async_remote_copy(
        src_ref=src,
        dst_ref=dst,
        send_sem=send,
        recv_sem=recv,
        device_id=peer,
        device_id_type=MESH,
    )


def at(index, size):
    return pl.ds(pl.multiple_of(index * size, size), size)


def body(
    nz,
    nx,
    source,
    target,
    source_gain,
    target_gain,
    query_weight,
    key_weight,
    value_weight,
    head_gain,
    out_weight,
    mlp_gain,
    gate_weight,
    up_weight,
    down_weight,
    out,
    src,
    tgt,
    wkv,
    wq,
    sgain,
    tgain,
    mgain,
    hgain,
    wo,
    wg,
    wu,
    wd,
    normed,
    kb,
    vb,
    qb,
    score,
    po,
    ps,
    pr,
    prs,
    ho,
    st,
    hid,
    part,
    pb,
    d2,
    comb,
    fr,
    mixed,
    lsem,
    src_s,
    src_r,
    ag_s,
    ag_r,
    w_s,
    w_r,
    k_s,
    k_r,
    q_s,
    q_r,
    p_s,
    p_r,
    d_s,
    d_r,
    f_s,
    f_r,
    o_s,
):
    ntp = 2 * nx
    depth = src.shape[1]
    src_rows = src.shape[0] // ntp
    own_rows = tgt.shape[0] // ntp
    rows = tgt.shape[0]
    block = src.shape[0]
    chunk = 2 * src_rows
    cols = depth // ntp
    hd = HEAD_DIM
    sp = lax.axis_index("sp")
    tp = lax.axis_index("tp")
    z = lax.div(sp, NY)
    y = lax.rem(sp, NY)
    x = lax.div(tp, 2)
    c = lax.rem(tp, 2)

    def device(zz, yy, xx, cc):
        return (zz * NY + yy, xx * 2 + cc)

    def x_peer(d):
        return device(z, y, lax.rem(x + d, nx), c)

    def y_peer(d):
        return device(z, lax.rem(y + d, NY), x, c)

    def z_peer(d):
        return device(lax.rem(z + d, nz), y, x, c)

    partner = device(z, y, x, 1 - c)
    x_order = (1, 3, 2) if nx == 4 else tuple(range(1, nx))

    loads = {}

    def load(name, index, source_ref, to):
        loads[name] = pltpu.make_async_copy(source_ref, to, lsem.at[index])
        loads[name].start()

    load("tgt", 0, target, tgt.at[at(tp, own_rows)])
    load("src", 1, source, src.at[at(tp, src_rows)])
    load("sgain", 2, source_gain, sgain)
    load("k", 3, key_weight, wkv.at[:, :, 0:hd])
    load("v", 4, value_weight, wkv.at[:, :, hd : 2 * hd])
    load("tgain", 5, target_gain, tgain)
    load("q", 6, query_weight, wq)
    load("hgain", 7, head_gain, hgain)
    load("mgain", 8, mlp_gain, mgain)
    load("wo0", 9, out_weight.at[0], wo.at[0, at(tp, hd)])
    load("wo1", 13, out_weight.at[1], wo.at[1, at(tp, hd)])
    load("wg", 10, gate_weight, wg)
    load("wu", 11, up_weight, wu)
    load("wd", 12, down_weight, wd)

    scope = jax.named_scope
    barrier = pltpu.get_barrier_semaphore()
    peers = [device(z, y, lax.rem(x + d // 2, nx), lax.rem(c + d, 2)) for d in range(1, ntp)]
    peers += [y_peer(d) for d in range(1, NY)]
    peers += [z_peer(d) for d in range(1, nz)]
    with scope("barrier"):
        for peer in peers:
            pl.semaphore_signal(barrier, inc=1, device_id=peer, device_id_type=MESH)
        pl.semaphore_wait(barrier, len(peers))

    def all_sent(ref, sem):
        rcopy(ref, ref, sem, sem, partner).wait_send()

    def all_here(ref, sem):
        rcopy(ref, ref, sem, sem, partner).wait_recv()

    class Gather:
        def __init__(self, index, view):
            self.view = view
            self.send = ag_s.at[index]
            self.near = ag_r.at[index, 0]
            mine = view(tp)
            self.first = {d: rcopy(mine, mine, self.send, ag_r.at[index, d], x_peer(d)) for d in x_order}
            rcopy(mine, mine, self.send, self.near, partner).start()
            for d in x_order:
                self.first[d].start()

        def forward(self):
            for d in x_order:
                self.first[d].wait_recv()
                there = self.view(lax.rem(x + nx - d, nx) * 2 + c)
                rcopy(there, there, self.send, self.near, partner).start()

        def finish(self, near_bytes, sent_bytes):
            all_here(near_bytes, self.near)
            all_sent(sent_bytes, self.send)

    left, right = x_peer(nx - 1), x_peer(1)
    tp_left = lax.rem(x + nx - 1, nx) * 2 + c
    tp_right = lax.rem(x + 1, nx) * 2 + c
    tp_far = lax.rem(x + 2, nx) * 2 + c

    class Spread:
        def __init__(self, ref, size, send, recv, near):
            self.ref, self.size, self.half = ref, size, size // 2
            self.send, self.recv, self.near = send, recv, near

        def copy(self, sem, owner, first, count, to):
            start = pl.multiple_of(owner * self.size + first, self.half)
            ref = self.ref.at[pl.ds(start, count)]
            rcopy(ref, ref, self.send, sem, to).start()

        def wait(self, index):
            all_here(self.ref.at[pl.ds(0, self.half)], self.recv.at[index])

        def start(self):
            half = self.half
            self.copy(self.near[0], tp, 0, self.size, partner)
            self.copy(self.recv.at[1], tp, 0, half, right)
            self.copy(self.recv.at[2], tp, half, half, left)
            self.copy(self.recv.at[3], tp, half, half, right)
            self.copy(self.recv.at[4], tp, 0, half, left)

        def relay(self):
            self.wait(1)
            self.copy(self.recv.at[5], tp_left, 0, self.half, right)
            self.wait(2)
            self.copy(self.recv.at[6], tp_right, self.half, self.half, left)

        def forward_sides(self):
            self.wait(3)
            self.copy(self.near[1], tp_left, 0, self.size, partner)
            self.wait(4)
            self.copy(self.near[2], tp_right, 0, self.size, partner)

        def forward_far(self):
            self.wait(5)
            self.copy(self.near[3], tp_far, 0, self.half, partner)
            self.wait(6)
            self.copy(self.near[4], tp_far, self.half, self.half, partner)

        def sent(self):
            all_sent(self.ref.at[0 : 7 * self.size], self.send)

    spread_src = Spread(src, src_rows, src_s, src_r, [src_r.at[i] for i in (0, 7, 8, 9, 10)])
    spread_wo = [
        Spread(wo.at[layer], hd, w_s.at[layer], w_r.at[layer], [w_r.at[layer, 0]] * 5)
        for layer in range(2)
    ]
    loads["src"].wait()
    spread_src.start()
    loads["tgt"].wait()
    gather_tgt = Gather(0, lambda j: tgt.at[at(j, own_rows)])

    def src_here(index, count):
        all_here(src.at[pl.ds(0, count)], src_r.at[index])

    factor = math.log2(math.e) * hd**-0.5

    def norm_rows(from_ref, start, count, gain_of):
        step = 64

        def one(i, carry):
            at_from = pl.ds(pl.multiple_of(start + i * step, step), step)
            at_to = pl.ds(pl.multiple_of(i * step, step), step)
            total = jnp.zeros((step, 128), F32)
            for k in range(0, depth, 128):
                v = from_ref[at_from, k : k + 128].astype(F32)
                total += v * v
            mean = jnp.sum(total, axis=1, keepdims=True) * (1.0 / depth)
            scale = lax.rsqrt(mean + EPSILON)
            for k in range(0, depth, 128):
                v = from_ref[at_from, k : k + 128].astype(F32)
                g = gain_of(k).astype(F32)
                normed[at_to, k : k + 128] = (v * scale * g).astype(BF16)
            return carry

        lax.fori_loop(0, count // step, one, 0)

    def project_source(layer, xx):
        norm_rows(src, xx * chunk, chunk, lambda k: sgain[layer : layer + 1, k : k + 128])
        kv = jnp.dot(normed[0:chunk], wkv[layer], preferred_element_type=F32)
        first = y * block + xx * chunk
        here = pl.ds(pl.multiple_of(first, chunk), chunk)
        kb[layer, here] = kv[:, 0:hd].astype(BF16)
        vb[layer, :, here] = jnp.transpose(kv[:, hd : 2 * hd]).astype(BF16)

    def k0_copies(xx, d):
        here = pl.ds(pl.multiple_of(y * block + xx * chunk, chunk), chunk)
        k = kb.at[0, here]
        v = vb.at[0, :, here]
        return (
            rcopy(k, k, k_s.at[0, 0], k_r.at[0, 0], y_peer(d)),
            rcopy(v, v, k_s.at[0, 1], k_r.at[0, 1], y_peer(d)),
        )

    def k1_copies(d):
        here = at(y, block)
        k = kb.at[1, here]
        v = vb.at[1, :, here]
        return (
            rcopy(k, k, k_s.at[1, 0], k_r.at[1, 0], y_peer(d)),
            rcopy(v, v, k_s.at[1, 1], k_r.at[1, 1], y_peer(d)),
        )

    def z_order(i):
        odd = lax.rem(i, 2)
        return odd * lax.div(i + 1, 2) + (1 - odd) * lax.rem(nz - lax.div(i, 2), nz)

    def q_copy(layer, slot, source_slot=0, d=None):
        to = z_peer(z_order(slot) if d is None else d)
        return rcopy(
            qb.at[layer, source_slot],
            qb.at[layer, slot],
            q_s.at[layer],
            q_r.at[layer, slot],
            to,
        )

    def project_query(layer, state_ref):
        norm_rows(state_ref, 0, rows, lambda k: tgain[layer : layer + 1, k : k + 128])
        q = jnp.dot(normed[0:rows], wq[layer], preferred_element_type=F32)
        qb[layer, 0] = (q * factor).astype(BF16)

        for slot in (3, 4, 1, 2):
            q_copy(layer, slot).start()

    def q_wait(layer, slot):
        q_copy(layer, slot).wait_recv()

    def relay_queries(layer):
        q_wait(layer, 3)
        q_copy(layer, 5, 3, 1).start()
        q_wait(layer, 4)
        q_copy(layer, 6, 4, nz - 1).start()
        q_copy(layer, 7, 3 + c, 2 + c * (nz - 4)).start()

    def send_k0(xx):
        for d in (1, 3, 2):
            for cp in k0_copies(xx, d):
                cp.start()

    with scope("wait_own"):
        loads["sgain"].wait()
        loads["k"].wait()
        loads["v"].wait()
        src_here(0, src_rows)
    with scope("kv_own"):
        project_source(0, x)
        send_k0(x)
    with scope("wait_src"):
        spread_src.relay()
        spread_src.forward_sides()
        src_here(7, src_rows)
    with scope("kv_left"):
        xx = lax.rem(x + nx - 1, nx)
        project_source(0, xx)
        send_k0(xx)
    src_here(8, src_rows)
    with scope("kv_right"):
        xx = lax.rem(x + 1, nx)
        project_source(0, xx)
        send_k0(xx)
    with scope("wait_tgt"):
        gather_tgt.forward()
        gather_tgt.finish(tgt.at[0 : 4 * own_rows], tgt.at[0 : 7 * own_rows])
        loads["tgain"].wait()
        loads["q"].wait()
    with scope("q0"):
        project_query(0, tgt)
    loads["wo0"].wait()
    spread_wo[0].start()
    with scope("wait_far"):
        spread_src.forward_far()
        src_here(9, src_rows // 2)
        src_here(10, src_rows // 2)
    with scope("kv_far"):
        xx = lax.rem(x + 2, nx)
        project_source(0, xx)
        send_k0(xx)

    def project_one(i, carry):
        project_source(1, i)
        return carry

    with scope("kv1"):
        lax.fori_loop(0, nx, project_one, 0)
    with scope("relay_q0"):
        relay_queries(0)
    for d in (1, 3, 2):
        for cp in k1_copies(d):
            cp.start()

    def p_copies(layer, slot):
        to = z_peer(nz - z_order(slot))
        return (
            rcopy(
                po.at[layer, slot], pr.at[layer, slot], p_s.at[layer, 0], p_r.at[layer, 0], to
            ),
            rcopy(
                ps.at[layer, slot], prs.at[layer, slot], p_s.at[layer, 1], p_r.at[layer, 1], to
            ),
        )

    def attend(layer, first, count):
        wide = count * rows
        q = qb[layer, pl.ds(first, count)].reshape(wide, hd)
        top = None
        for b in range(NY):
            here = slice(b * block, (b + 1) * block)
            s = lax.dot_general(
                kb[layer, here], q, (((1,), (1,)), ((), ())), preferred_element_type=F32
            )
            score[here, 0:wide] = s
            m = jnp.max(s, axis=0, keepdims=True)
            top = m if top is None else jnp.maximum(top, m)
        total = jnp.zeros((1, wide), F32)
        acc = jnp.zeros((hd, wide), F32)
        for b in range(NY):
            here = slice(b * block, (b + 1) * block)
            w = jnp.exp2(score[here, 0:wide] - top)
            total += jnp.sum(w, axis=0, keepdims=True)
            acc += jnp.dot(vb[layer, :, here], w.astype(BF16), preferred_element_type=F32)
        low = acc.astype(BF16)
        which = lax.broadcasted_iota(jnp.int32, (8, wide), 0)
        stats = jnp.where(which == 0, top, total)
        for j in range(count):
            to_out, to_stats = (pr, prs) if isinstance(first, int) and first == 0 else (po, ps)
            to_out[layer, first + j] = low[:, j * rows : (j + 1) * rows]
            to_stats[layer, first + j] = stats[:, j * rows : (j + 1) * rows]
            if to_out is po:
                for cp in p_copies(layer, first + j):
                    cp.start()

    def attend_first():
        for slot in (1, 2, 5, 6, 7):
            q_wait(0, slot)
        attend(0, nz - 1, 1)

        def pair(i, carry):
            attend(0, nz - 3 - 2 * i, 2)
            return carry

        lax.fori_loop(0, (nz - 2) // 2, pair, 0)
        attend(0, 0, 1)

    def attend_second():
        attend(1, 0, 1)
        with scope("relay_q1"):
            relay_queries(1)
        with scope("wait_q"):
            q_wait(1, 1)
            q_wait(1, 2)
        attend(1, 1, 2)
        with scope("relay_wo1"):
            spread_wo[1].relay()
        attend(1, 3, 2)
        with scope("wait_q"):
            q_wait(1, 5)
            q_wait(1, 6)
        attend(1, 5, 2)
        with scope("wait_q"):
            q_wait(1, 7)
        attend(1, 7, 1)

    def merge(layer):
        with scope("wait_p"):
            all_here(pr.at[layer, 1:nz], p_r.at[layer, 0])
            all_here(prs.at[layer, 1:nz], p_r.at[layer, 1])
        top = prs[layer, 0, 0:1]
        for d in range(1, nz):
            top = jnp.maximum(top, prs[layer, d, 0:1])
        total = jnp.zeros((1, rows), F32)
        acc = jnp.zeros((hd, rows), F32)
        for d in range(nz):
            f = jnp.exp2(prs[layer, d, 0:1] - top)
            total += f * prs[layer, d, 1:2]
            acc += f * pr[layer, d].astype(F32)
        attended = acc / total
        mean = jnp.mean(attended * attended, axis=0, keepdims=True)
        scaled = jnp.transpose(attended * lax.rsqrt(mean + EPSILON))
        gain = hgain[layer : layer + 1, :].astype(F32)
        ho[layer, :, at(tp, hd)] = (scaled * gain).astype(BF16)

    def gather_heads(layer):
        with scope("gather_ho"):
            gather = Gather(1 + layer, lambda j: ho.at[layer, :, at(j, hd)])
            spread_wo[layer].forward_far()
            gather.forward()
            gather.finish(ho.at[layer, :, 0 : 4 * hd], ho.at[layer, :, 0 : 7 * hd])

    def project_heads(layer, old):
        with scope("wait_wo"):
            all_here(wo.at[layer, 0 : 4 * hd], w_r.at[layer, 0])
        with scope("out"):

            def out_piece(i, carry):
                w = at(i, 512)
                add = jnp.dot(ho[layer], wo[layer, :, w], preferred_element_type=F32)
                st[layer, :, w] = (old[:, w].astype(F32) + add).astype(BF16)
                return carry

            lax.fori_loop(0, depth // 512, out_piece, 0)

    def kv_wait(layer):
        most = (NY - 1) * block
        all_here(kb.at[layer, 0:most], k_r.at[layer, 0])
        all_here(vb.at[layer, :, 0:most], k_r.at[layer, 1])

    with scope("wait_kv0"):
        kv_wait(0)
    with scope("relay_wo0"):
        spread_wo[0].relay()
    with scope("attend0"):
        attend_first()
    with scope("sides_wo0"):
        spread_wo[0].forward_sides()
    loads["hgain"].wait()
    with scope("merge0"):
        merge(0)
    gather_heads(0)
    loads["wo1"].wait()
    spread_wo[1].start()
    project_heads(0, tgt)
    with scope("q1"):
        project_query(1, st.at[0])
    with scope("wait_kv1"):
        kv_wait(1)
    with scope("attend1"):
        attend_second()
    with scope("sides_wo1"):
        spread_wo[1].forward_sides()
    with scope("merge1"):
        merge(1)
    gather_heads(1)
    project_heads(1, st.at[0])

    loads["mgain"].wait()
    loads["wg"].wait()
    loads["wu"].wait()
    loads["wd"].wait()
    with scope("mlp_norm"):
        norm_rows(st.at[1], 0, rows, lambda k: mgain[k // 128 : k // 128 + 1, :])
    over = (((1,), (1,)), ((), ()))
    with scope("gate"):
        gate = lax.dot_general(wg[...], normed[0:rows], over, preferred_element_type=F32)
        up = lax.dot_general(wu[...], normed[0:rows], over, preferred_element_type=F32)
        hid[...] = jnp.transpose(gate / (1.0 + jnp.exp(-gate)) * up).astype(BF16)
    pieces = 4
    width = depth // pieces

    def d2_copy(n):
        w = slice(n * width, (n + 1) * width)
        return rcopy(pb.at[:, :, w], d2.at[:, :, w], d_s, d_r.at[n], partner)

    def fr_copy(n, d):
        w = slice(n * width, (n + 1) * width)
        return rcopy(comb.at[d, :, w], fr.at[d, :, w], f_s, f_r.at[n], x_peer(d))

    def pair_sum(n):
        w = slice(n * width, (n + 1) * width)
        with scope("wait_d2"):
            d2_copy(n).wait_recv()
        for d in x_order:
            xx = lax.rem(x + d, nx)
            comb[d, :, w] = (part[xx, c, :, w] + d2[xx, :, w].astype(F32)).astype(BF16)
            fr_copy(n, d).start()

    for n in range(pieces):
        w = slice(n * width, (n + 1) * width)
        with scope("down"):
            down = jnp.dot(hid[...], wd[:, w], preferred_element_type=F32)
            part[:, :, :, w] = down.reshape(nx, 2, own_rows, width)
            pb[:, :, w] = part[:, 1 - c, :, w].astype(BF16)
            d2_copy(n).start()
        if n > 0:
            pair_sum(n - 1)
    pair_sum(pieces - 1)
    def out_piece_copy(n):
        w = slice(n * width, (n + 1) * width)
        return pltpu.make_async_copy(mixed.at[:, w], out.at[:, w], o_s)

    for n in range(pieces):
        w = slice(n * width, (n + 1) * width)
        down = part[x, c, :, w] + d2[x, :, w].astype(F32)
        with scope("wait_fr"):
            all_here(fr.at[1:nx, :, w], f_r.at[n])
        for d in x_order:
            down += fr[d, :, w].astype(F32)
        state = st[1, at(tp, own_rows), w].astype(F32)
        mixed[:, w] = (state + 0.5 * down).astype(BF16)
        out_piece_copy(n).start()

    with scope("drain"):
        spread_src.sent()
        for spread in spread_wo:
            spread.sent()
        for layer in range(2):
            all_sent(kb.at[layer, 0 : (NY - 1) * block], k_s.at[layer, 0])
            all_sent(vb.at[layer, :, 0 : (NY - 1) * block], k_s.at[layer, 1])
            all_sent(qb.at[layer, 1:nz], q_s.at[layer])
            all_sent(po.at[layer, 1:nz], p_s.at[layer, 0])
            all_sent(ps.at[layer, 1:nz], p_s.at[layer, 1])
        all_sent(pb, d_s)
        all_sent(comb.at[1:nx], f_s)
        pltpu.make_async_copy(mixed, out, o_s).wait()


def local(nz, nx, *args):
    source, target = args[0], args[1]
    ntp = 2 * nx
    depth = source.shape[1]
    block = source.shape[0] * ntp
    rows = target.shape[0] * ntp
    own = target.shape[0]
    ffl = args[10].shape[1]
    hd = HEAD_DIM
    args = list(args)
    args[9] = args[9].reshape(depth // 128, 128)
    args[10] = args[10].T
    args[11] = args[11].T
    vmem = pltpu.VMEM
    dma = pltpu.SemaphoreType.DMA
    scratch = [
        vmem((block, depth), BF16),
        vmem((rows, depth), BF16),
        vmem((2, depth, 2 * hd), BF16),
        vmem((2, depth, hd), BF16),
        vmem((2, depth), BF16),
        vmem((2, depth), BF16),
        vmem((depth // 128, 128), BF16),
        vmem((2, hd), BF16),
        vmem((2, ntp * hd, depth), BF16),
        vmem((ffl, depth), BF16),
        vmem((ffl, depth), BF16),
        vmem((ffl, depth), BF16),
        vmem((rows, depth), BF16),
        vmem((2, NY * block, hd), BF16),
        vmem((2, hd, NY * block), BF16),
        vmem((2, nz, rows, hd), BF16),
        vmem((NY * block, 2 * rows), F32),
        vmem((2, nz, hd, rows), BF16),
        vmem((2, nz, 8, rows), F32),
        vmem((2, nz, hd, rows), BF16),
        vmem((2, nz, 8, rows), F32),
        vmem((2, rows, ntp * hd), BF16),
        vmem((2, rows, depth), BF16),
        vmem((rows, ffl), BF16),
        vmem((nx, 2, own, depth), F32),
        vmem((nx, own, depth), BF16),
        vmem((nx, own, depth), BF16),
        vmem((nx, own, depth), BF16),
        vmem((nx, own, depth), BF16),
        vmem((own, depth), BF16),
        dma((14,)),
        dma(()),
        dma((11,)),
        dma((3,)),
        dma((3, nx)),
        dma((2,)),
        dma((2, 7)),
        dma((2, 2)),
        dma((2, 2)),
        dma((2,)),
        dma((2, nz)),
        dma((2, 2)),
        dma((2, 2)),
        dma(()),
        dma((4,)),
        dma(()),
        dma((4,)),
        dma(()),
    ]
    return pl.pallas_call(
        functools.partial(body, nz, nx),
        name="decoder",
        out_shape=jax.ShapeDtypeStruct(target.shape, BF16),
        in_specs=[pl.BlockSpec(memory_space=pl.ANY)] * len(args),
        out_specs=pl.BlockSpec(memory_space=pl.ANY),
        scratch_shapes=scratch,
        compiler_params=pltpu.CompilerParams(
            collective_id=0, has_side_effects=True, vmem_limit_bytes=60 * 1024 * 1024
        ),
    )(*args)


def solution(mesh):
    nz = mesh.shape["sp"] // NY
    nx = mesh.shape["tp"] // 2
    in_specs = (
        P(("sp", "tp"), None),
        P(("sp", "tp"), None),
        P(),
        P(),
        P(None, None, "tp"),
        P(None, None, "tp"),
        P(None, None, "tp"),
        P(None, "tp"),
        P(None, "tp", None),
        P(),
        P(None, "tp"),
        P(None, "tp"),
        P("tp", None),
    )
    out_specs = P(("sp", "tp"), None)
    return jax.shard_map(
        functools.partial(local, nz, nx),
        mesh=mesh,
        in_specs=in_specs,
        out_specs=out_specs,
        check_vma=False,
    )
```

```python
import functools
import math

import jax
import jax.numpy as jnp
from jax import lax
from jax.experimental import pallas as pl
from jax.experimental.pallas import tpu as pltpu
from jax.sharding import PartitionSpec as P

HEAD_DIM = 128
EPSILON = 1e-06
NY = 4
MESH = pl.DeviceIdType.MESH
BF16 = jnp.bfloat16
F32 = jnp.float32


def rcopy(src, dst, send, recv, peer):
    return pltpu.make_async_remote_copy(
        src_ref=src,
        dst_ref=dst,
        send_sem=send,
        recv_sem=recv,
        device_id=peer,
        device_id_type=MESH,
    )


def at(index, size):
    return pl.ds(pl.multiple_of(index * size, size), size)


def body(
    nz,
    nx,
    source,
    target,
    source_gain,
    target_gain,
    query_weight,
    key_weight,
    value_weight,
    head_gain,
    out_weight,
    mlp_gain,
    gate_weight,
    up_weight,
    down_weight,
    out,
    src,
    tgt,
    wkv,
    wq,
    sgain,
    tgain,
    mgain,
    hgain,
    wo,
    wg,
    wu,
    wd,
    normed,
    kb,
    vb,
    qb,
    score,
    po,
    ps,
    pr,
    prs,
    ho,
    st,
    hid,
    part,
    pb,
    d2,
    comb,
    fr,
    mixed,
    lsem,
    src_s,
    src_r,
    ag_s,
    ag_r,
    w_s,
    w_r,
    k_s,
    k_r,
    k0_r,
    q_s,
    q_r,
    p_s,
    p_r,
    d_s,
    d_r,
    f_s,
    f_r,
    o_s,
):
    ntp = 2 * nx
    depth = src.shape[1]
    src_rows = src.shape[0] // ntp
    own_rows = tgt.shape[0] // ntp
    rows = tgt.shape[0]
    block = src.shape[0]
    chunk = 2 * src_rows
    cols = depth // ntp
    hd = HEAD_DIM
    sp = lax.axis_index("sp")
    tp = lax.axis_index("tp")
    z = lax.div(sp, NY)
    y = lax.rem(sp, NY)
    x = lax.div(tp, 2)
    c = lax.rem(tp, 2)

    def device(zz, yy, xx, cc):
        return (zz * NY + yy, xx * 2 + cc)

    def x_peer(d):
        return device(z, y, lax.rem(x + d, nx), c)

    def y_peer(d):
        return device(z, lax.rem(y + d, NY), x, c)

    def z_peer(d):
        return device(lax.rem(z + d, nz), y, x, c)

    partner = device(z, y, x, 1 - c)
    x_order = (1, 3, 2) if nx == 4 else tuple(range(1, nx))

    loads = {}

    def load(name, index, source_ref, to):
        loads[name] = pltpu.make_async_copy(source_ref, to, lsem.at[index])
        loads[name].start()

    load("tgt", 0, target, tgt.at[at(tp, own_rows)])
    load("src", 1, source, src.at[at(tp, src_rows)])
    load("sgain", 2, source_gain, sgain)
    load("k", 3, key_weight, wkv.at[:, :, 0:hd])
    load("v", 4, value_weight, wkv.at[:, :, hd : 2 * hd])
    load("tgain", 5, target_gain, tgain)
    load("q", 6, query_weight, wq)
    load("hgain", 7, head_gain, hgain)
    load("mgain", 8, mlp_gain, mgain)
    load("wo0", 9, out_weight.at[0], wo.at[0, at(tp, hd)])
    load("wo1", 13, out_weight.at[1], wo.at[1, at(tp, hd)])
    load("wg", 10, gate_weight, wg)
    load("wu", 11, up_weight, wu)
    load("wd", 12, down_weight, wd)

    scope = jax.named_scope
    barrier = pltpu.get_barrier_semaphore()
    peers = [device(z, y, lax.rem(x + d // 2, nx), lax.rem(c + d, 2)) for d in range(1, ntp)]
    peers += [y_peer(d) for d in range(1, NY)]
    peers += [z_peer(d) for d in range(1, nz)]
    with scope("barrier"):
        for peer in peers:
            pl.semaphore_signal(barrier, inc=1, device_id=peer, device_id_type=MESH)
        pl.semaphore_wait(barrier, len(peers))

    def all_sent(ref, sem):
        rcopy(ref, ref, sem, sem, partner).wait_send()

    def all_here(ref, sem):
        rcopy(ref, ref, sem, sem, partner).wait_recv()

    class Gather:
        def __init__(self, index, view):
            self.view = view
            self.send = ag_s.at[index]
            self.near = ag_r.at[index, 0]
            mine = view(tp)
            self.first = {d: rcopy(mine, mine, self.send, ag_r.at[index, d], x_peer(d)) for d in x_order}
            rcopy(mine, mine, self.send, self.near, partner).start()
            for d in x_order:
                self.first[d].start()

        def forward(self):
            for d in x_order:
                self.first[d].wait_recv()
                there = self.view(lax.rem(x + nx - d, nx) * 2 + c)
                rcopy(there, there, self.send, self.near, partner).start()

        def finish(self, near_bytes, sent_bytes):
            all_here(near_bytes, self.near)
            all_sent(sent_bytes, self.send)

    left, right = x_peer(nx - 1), x_peer(1)
    tp_left = lax.rem(x + nx - 1, nx) * 2 + c
    tp_right = lax.rem(x + 1, nx) * 2 + c
    tp_far = lax.rem(x + 2, nx) * 2 + c

    class Spread:
        def __init__(self, ref, size, send, recv, near):
            self.ref, self.size, self.half = ref, size, size // 2
            self.send, self.recv, self.near = send, recv, near

        def copy(self, sem, owner, first, count, to):
            start = pl.multiple_of(owner * self.size + first, self.half)
            ref = self.ref.at[pl.ds(start, count)]
            rcopy(ref, ref, self.send, sem, to).start()

        def wait(self, index):
            all_here(self.ref.at[pl.ds(0, self.half)], self.recv.at[index])

        def start(self):
            half = self.half
            self.copy(self.near[0], tp, 0, self.size, partner)
            self.copy(self.recv.at[1], tp, 0, half, right)
            self.copy(self.recv.at[2], tp, half, half, left)
            self.copy(self.recv.at[3], tp, half, half, right)
            self.copy(self.recv.at[4], tp, 0, half, left)

        def relay(self):
            self.wait(1)
            self.copy(self.recv.at[5], tp_left, 0, self.half, right)
            self.wait(2)
            self.copy(self.recv.at[6], tp_right, self.half, self.half, left)

        def forward_sides(self):
            self.wait(3)
            self.copy(self.near[1], tp_left, 0, self.size, partner)
            self.wait(4)
            self.copy(self.near[2], tp_right, 0, self.size, partner)

        def forward_far(self):
            self.wait(5)
            self.copy(self.near[3], tp_far, 0, self.half, partner)
            self.wait(6)
            self.copy(self.near[4], tp_far, self.half, self.half, partner)

        def sent(self):
            all_sent(self.ref.at[0 : 7 * self.size], self.send)

    spread_src = Spread(src, src_rows, src_s, src_r, [src_r.at[i] for i in (0, 7, 8, 9, 10)])
    spread_wo = [
        Spread(wo.at[layer], hd, w_s.at[layer], w_r.at[layer], [w_r.at[layer, 0]] * 5)
        for layer in range(2)
    ]
    loads["src"].wait()
    spread_src.start()

    def src_here(index, count):
        all_here(src.at[pl.ds(0, count)], src_r.at[index])

    factor = math.log2(math.e) * hd**-0.5

    def norm_rows(from_ref, start, count, gain_of):
        step = 64

        def one(i, carry):
            at_from = pl.ds(pl.multiple_of(start + i * step, step), step)
            at_to = pl.ds(pl.multiple_of(i * step, step), step)
            total = jnp.zeros((step, 128), F32)
            for k in range(0, depth, 128):
                v = from_ref[at_from, k : k + 128].astype(F32)
                total += v * v
            mean = jnp.sum(total, axis=1, keepdims=True) * (1.0 / depth)
            scale = lax.rsqrt(mean + EPSILON)
            for k in range(0, depth, 128):
                v = from_ref[at_from, k : k + 128].astype(F32)
                g = gain_of(k).astype(F32)
                normed[at_to, k : k + 128] = (v * scale * g).astype(BF16)
            return carry

        lax.fori_loop(0, count // step, one, 0)

    def project_source(layer, xx):
        norm_rows(src, xx * chunk, chunk, lambda k: sgain[layer : layer + 1, k : k + 128])
        kv = jnp.dot(normed[0:chunk], wkv[layer], preferred_element_type=F32)
        first = y * block + xx * chunk
        here = pl.ds(pl.multiple_of(first, chunk), chunk)
        kb[layer, here] = kv[:, 0:hd].astype(BF16)
        vb[layer, :, here] = jnp.transpose(kv[:, hd : 2 * hd]).astype(BF16)

    def k0_copy(kind, yy, xx, recv, to):
        here = pl.ds(pl.multiple_of(yy * block + xx * chunk, chunk), chunk)
        ref = vb.at[0, :, here] if kind else kb.at[0, here]
        return rcopy(ref, ref, k_s.at[0, kind], recv, to)

    def send_k0(xx):
        after, before = y_peer(1), y_peer(NY - 1)
        k0_copy(0, y, xx, k0_r.at[0, xx], after).start()
        k0_copy(1, y, xx, k0_r.at[1, xx], before).start()
        k0_copy(0, y, xx, k_r.at[0, 0], before).start()
        k0_copy(1, y, xx, k_r.at[0, 1], after).start()

    def relay_k0(xx):
        after, before = y_peer(1), y_peer(NY - 1)
        k0_copy(0, y, xx, k0_r.at[0, xx], after).wait_recv()
        k0_copy(0, lax.rem(y + NY - 1, NY), xx, k_r.at[0, 0], after).start()
        k0_copy(1, y, xx, k0_r.at[1, xx], before).wait_recv()
        k0_copy(1, lax.rem(y + 1, NY), xx, k_r.at[0, 1], before).start()

    def k1_copies(d):
        here = at(y, block)
        k = kb.at[1, here]
        v = vb.at[1, :, here]
        return (
            rcopy(k, k, k_s.at[1, 0], k_r.at[1, 0], y_peer(d)),
            rcopy(v, v, k_s.at[1, 1], k_r.at[1, 1], y_peer(d)),
        )

    def z_order(i):
        odd = lax.rem(i, 2)
        return odd * lax.div(i + 1, 2) + (1 - odd) * lax.rem(nz - lax.div(i, 2), nz)

    def q_copy(layer, slot, source_slot=0, d=None):
        to = z_peer(z_order(slot) if d is None else d)
        return rcopy(
            qb.at[layer, source_slot],
            qb.at[layer, slot],
            q_s.at[layer],
            q_r.at[layer, slot],
            to,
        )

    def project_query(layer, state_ref):
        norm_rows(state_ref, 0, rows, lambda k: tgain[layer : layer + 1, k : k + 128])
        q = jnp.dot(normed[0:rows], wq[layer], preferred_element_type=F32)
        qb[layer, 0] = (q * factor).astype(BF16)

        for slot in (3, 4, 1, 2):
            q_copy(layer, slot).start()

    def q_wait(layer, slot):
        q_copy(layer, slot).wait_recv()

    def relay_queries(layer):
        q_wait(layer, 3)
        q_copy(layer, 5, 3, 1).start()
        q_wait(layer, 4)
        q_copy(layer, 6, 4, nz - 1).start()
        q_copy(layer, 7, 3 + c, 2 + c * (nz - 4)).start()

    with scope("wait_own"):
        loads["sgain"].wait()
        loads["k"].wait()
        loads["v"].wait()
        src_here(0, src_rows)
    with scope("kv_own"):
        project_source(0, x)
        send_k0(x)
    with scope("wait_src"):
        spread_src.relay()
        loads["tgt"].wait()
        gather_tgt = Gather(0, lambda j: tgt.at[at(j, own_rows)])
        spread_src.forward_sides()
        src_here(7, src_rows)
    x_left, x_right, x_far = (lax.rem(x + d, nx) for d in (nx - 1, 1, 2))
    with scope("relay_k0"):
        relay_k0(x)
    with scope("kv_left"):
        project_source(0, x_left)
        send_k0(x_left)
    src_here(8, src_rows)
    with scope("kv_right"):
        project_source(0, x_right)
        send_k0(x_right)
    with scope("wait_far"):
        spread_src.forward_far()
        src_here(9, src_rows // 2)
        src_here(10, src_rows // 2)
    with scope("pass_tgt"):
        gather_tgt.forward()
    loads["wo0"].wait()
    spread_wo[0].start()
    with scope("kv_far"):
        project_source(0, x_far)
        send_k0(x_far)
    with scope("wait_tgt"):
        gather_tgt.finish(tgt.at[0 : 4 * own_rows], tgt.at[0 : 7 * own_rows])
        loads["tgain"].wait()
        loads["q"].wait()
    with scope("q0"):
        project_query(0, tgt)
    with scope("relay_k0"):
        relay_k0(x_left)
        relay_k0(x_right)

    def project_one(i, carry):
        project_source(1, i)
        return carry

    with scope("kv1"):
        lax.fori_loop(0, nx // 2, project_one, 0)
    with scope("relay_k0"):
        relay_k0(x_far)
    with scope("kv1"):
        lax.fori_loop(nx // 2, nx, project_one, 0)
    with scope("relay_q0"):
        relay_queries(0)
    for d in (1, 3, 2):
        for cp in k1_copies(d):
            cp.start()

    def p_copies(layer, slot):
        to = z_peer(nz - z_order(slot))
        return (
            rcopy(
                po.at[layer, slot], pr.at[layer, slot], p_s.at[layer, 0], p_r.at[layer, 0], to
            ),
            rcopy(
                ps.at[layer, slot], prs.at[layer, slot], p_s.at[layer, 1], p_r.at[layer, 1], to
            ),
        )

    def attend(layer, first, count):
        wide = count * rows
        q = qb[layer, pl.ds(first, count)].reshape(wide, hd)
        top = None
        for b in range(NY):
            here = slice(b * block, (b + 1) * block)
            s = lax.dot_general(
                kb[layer, here], q, (((1,), (1,)), ((), ())), preferred_element_type=F32
            )
            score[here, 0:wide] = s
            m = jnp.max(s, axis=0, keepdims=True)
            top = m if top is None else jnp.maximum(top, m)
        total = jnp.zeros((1, wide), F32)
        acc = jnp.zeros((hd, wide), F32)
        for b in range(NY):
            here = slice(b * block, (b + 1) * block)
            w = jnp.exp2(score[here, 0:wide] - top)
            total += jnp.sum(w, axis=0, keepdims=True)
            acc += jnp.dot(vb[layer, :, here], w.astype(BF16), preferred_element_type=F32)
        low = acc.astype(BF16)
        which = lax.broadcasted_iota(jnp.int32, (8, wide), 0)
        stats = jnp.where(which == 0, top, total)
        for j in range(count):
            to_out, to_stats = (pr, prs) if isinstance(first, int) and first == 0 else (po, ps)
            to_out[layer, first + j] = low[:, j * rows : (j + 1) * rows]
            to_stats[layer, first + j] = stats[:, j * rows : (j + 1) * rows]
            if to_out is po:
                for cp in p_copies(layer, first + j):
                    cp.start()

    def attend_first():
        attend(0, 3, 2)
        q_wait(0, 1)
        q_wait(0, 2)
        attend(0, 1, 2)
        with scope("wait_q"):
            q_wait(0, 7)
        attend(0, 7, 1)
        q_wait(0, 5)
        q_wait(0, 6)
        attend(0, 5, 2)
        attend(0, 0, 1)

    def attend_second():
        attend(1, 0, 1)
        with scope("relay_q1"):
            relay_queries(1)
        with scope("wait_q"):
            q_wait(1, 1)
            q_wait(1, 2)
        attend(1, 1, 2)
        attend(1, 3, 2)
        with scope("relay_wo1"):
            spread_wo[1].relay()
        with scope("wait_q"):
            q_wait(1, 7)
        attend(1, 7, 1)
        with scope("wait_q"):
            q_wait(1, 5)
            q_wait(1, 6)
        attend(1, 5, 2)

    def merge(layer):
        with scope("wait_p"):
            all_here(pr.at[layer, 1:nz], p_r.at[layer, 0])
            all_here(prs.at[layer, 1:nz], p_r.at[layer, 1])
        top = prs[layer, 0, 0:1]
        for d in range(1, nz):
            top = jnp.maximum(top, prs[layer, d, 0:1])
        total = jnp.zeros((1, rows), F32)
        acc = jnp.zeros((hd, rows), F32)
        for d in range(nz):
            f = jnp.exp2(prs[layer, d, 0:1] - top)
            total += f * prs[layer, d, 1:2]
            acc += f * pr[layer, d].astype(F32)
        attended = acc / total
        mean = jnp.mean(attended * attended, axis=0, keepdims=True)
        scaled = jnp.transpose(attended * lax.rsqrt(mean + EPSILON))
        gain = hgain[layer : layer + 1, :].astype(F32)
        ho[layer, :, at(tp, hd)] = (scaled * gain).astype(BF16)

    def gather_heads(layer):
        with scope("gather_ho"):
            gather = Gather(1 + layer, lambda j: ho.at[layer, :, at(j, hd)])
            spread_wo[layer].forward_far()
            gather.forward()
            gather.finish(ho.at[layer, :, 0 : 4 * hd], ho.at[layer, :, 0 : 7 * hd])

    def project_heads(layer, old):
        with scope("wait_wo"):
            all_here(wo.at[layer, 0 : 4 * hd], w_r.at[layer, 0])
        with scope("out"):

            def out_piece(i, carry):
                w = at(i, 512)
                add = jnp.dot(ho[layer], wo[layer, :, w], preferred_element_type=F32)
                st[layer, :, w] = (old[:, w].astype(F32) + add).astype(BF16)
                return carry

            lax.fori_loop(0, depth // 512, out_piece, 0)

    def kv_wait(layer):
        most = (NY - 1 - (layer == 0)) * block
        all_here(kb.at[layer, 0:most], k_r.at[layer, 0])
        all_here(vb.at[layer, :, 0:most], k_r.at[layer, 1])

    with scope("wait_kv0"):
        kv_wait(0)
    with scope("relay_wo0"):
        spread_wo[0].relay()
    with scope("attend0"):
        attend_first()
    with scope("sides_wo0"):
        spread_wo[0].forward_sides()
    loads["hgain"].wait()
    with scope("merge0"):
        merge(0)
    gather_heads(0)
    loads["wo1"].wait()
    spread_wo[1].start()
    project_heads(0, tgt)
    with scope("q1"):
        project_query(1, st.at[0])
    with scope("wait_kv1"):
        kv_wait(1)
    with scope("attend1"):
        attend_second()
    with scope("sides_wo1"):
        spread_wo[1].forward_sides()
    with scope("merge1"):
        merge(1)
    gather_heads(1)
    project_heads(1, st.at[0])

    loads["mgain"].wait()
    loads["wg"].wait()
    loads["wu"].wait()
    loads["wd"].wait()
    with scope("mlp_norm"):
        norm_rows(st.at[1], 0, rows, lambda k: mgain[k // 128 : k // 128 + 1, :])
    over = (((1,), (1,)), ((), ()))
    with scope("gate"):
        gate = lax.dot_general(wg[...], normed[0:rows], over, preferred_element_type=F32)
        up = lax.dot_general(wu[...], normed[0:rows], over, preferred_element_type=F32)
        hid[...] = jnp.transpose(gate / (1.0 + jnp.exp(-gate)) * up).astype(BF16)
    pieces = 4
    width = depth // pieces

    def d2_copy(n):
        w = slice(n * width, (n + 1) * width)
        return rcopy(pb.at[:, :, w], d2.at[:, :, w], d_s, d_r.at[n], partner)

    def fr_copy(n, d):
        w = slice(n * width, (n + 1) * width)
        return rcopy(comb.at[d, :, w], fr.at[d, :, w], f_s, f_r.at[n], x_peer(d))

    def pair_sum(n):
        w = slice(n * width, (n + 1) * width)
        with scope("wait_d2"):
            d2_copy(n).wait_recv()
        for d in x_order:
            xx = lax.rem(x + d, nx)
            comb[d, :, w] = (part[xx, c, :, w] + d2[xx, :, w].astype(F32)).astype(BF16)
            fr_copy(n, d).start()

    for n in range(pieces):
        w = slice(n * width, (n + 1) * width)
        with scope("down"):
            down = jnp.dot(hid[...], wd[:, w], preferred_element_type=F32)
            part[:, :, :, w] = down.reshape(nx, 2, own_rows, width)
            pb[:, :, w] = part[:, 1 - c, :, w].astype(BF16)
            d2_copy(n).start()
        if n > 0:
            pair_sum(n - 1)
    pair_sum(pieces - 1)
    def out_piece_copy(n):
        w = slice(n * width, (n + 1) * width)
        return pltpu.make_async_copy(mixed.at[:, w], out.at[:, w], o_s)

    for n in range(pieces):
        w = slice(n * width, (n + 1) * width)
        down = part[x, c, :, w] + d2[x, :, w].astype(F32)
        with scope("wait_fr"):
            all_here(fr.at[1:nx, :, w], f_r.at[n])
        for d in x_order:
            down += fr[d, :, w].astype(F32)
        state = st[1, at(tp, own_rows), w].astype(F32)
        mixed[:, w] = (state + 0.5 * down).astype(BF16)
        out_piece_copy(n).start()

    with scope("drain"):
        spread_src.sent()
        for spread in spread_wo:
            spread.sent()
        for layer in range(2):
            all_sent(kb.at[layer, 0 : (NY - 1) * block], k_s.at[layer, 0])
            all_sent(vb.at[layer, :, 0 : (NY - 1) * block], k_s.at[layer, 1])
            all_sent(qb.at[layer, 1:nz], q_s.at[layer])
            all_sent(po.at[layer, 1:nz], p_s.at[layer, 0])
            all_sent(ps.at[layer, 1:nz], p_s.at[layer, 1])
        all_sent(pb, d_s)
        all_sent(comb.at[1:nx], f_s)
        pltpu.make_async_copy(mixed, out, o_s).wait()


def local(nz, nx, *args):
    source, target = args[0], args[1]
    ntp = 2 * nx
    depth = source.shape[1]
    block = source.shape[0] * ntp
    rows = target.shape[0] * ntp
    own = target.shape[0]
    ffl = args[10].shape[1]
    hd = HEAD_DIM
    args = list(args)
    args[9] = args[9].reshape(depth // 128, 128)
    args[10] = args[10].T
    args[11] = args[11].T
    vmem = pltpu.VMEM
    dma = pltpu.SemaphoreType.DMA
    scratch = [
        vmem((block, depth), BF16),
        vmem((rows, depth), BF16),
        vmem((2, depth, 2 * hd), BF16),
        vmem((2, depth, hd), BF16),
        vmem((2, depth), BF16),
        vmem((2, depth), BF16),
        vmem((depth // 128, 128), BF16),
        vmem((2, hd), BF16),
        vmem((2, ntp * hd, depth), BF16),
        vmem((ffl, depth), BF16),
        vmem((ffl, depth), BF16),
        vmem((ffl, depth), BF16),
        vmem((rows, depth), BF16),
        vmem((2, NY * block, hd), BF16),
        vmem((2, hd, NY * block), BF16),
        vmem((2, nz, rows, hd), BF16),
        vmem((NY * block, 2 * rows), F32),
        vmem((2, nz, hd, rows), BF16),
        vmem((2, nz, 8, rows), F32),
        vmem((2, nz, hd, rows), BF16),
        vmem((2, nz, 8, rows), F32),
        vmem((2, rows, ntp * hd), BF16),
        vmem((2, rows, depth), BF16),
        vmem((rows, ffl), BF16),
        vmem((nx, 2, own, depth), F32),
        vmem((nx, own, depth), BF16),
        vmem((nx, own, depth), BF16),
        vmem((nx, own, depth), BF16),
        vmem((nx, own, depth), BF16),
        vmem((own, depth), BF16),
        dma((14,)),
        dma(()),
        dma((11,)),
        dma((3,)),
        dma((3, nx)),
        dma((2,)),
        dma((2, 7)),
        dma((2, 2)),
        dma((2, 2)),
        dma((2, nx)),
        dma((2,)),
        dma((2, nz)),
        dma((2, 2)),
        dma((2, 2)),
        dma(()),
        dma((4,)),
        dma(()),
        dma((4,)),
        dma(()),
    ]
    return pl.pallas_call(
        functools.partial(body, nz, nx),
        name="decoder",
        out_shape=jax.ShapeDtypeStruct(target.shape, BF16),
        in_specs=[pl.BlockSpec(memory_space=pl.ANY)] * len(args),
        out_specs=pl.BlockSpec(memory_space=pl.ANY),
        scratch_shapes=scratch,
        compiler_params=pltpu.CompilerParams(
            collective_id=0, has_side_effects=True, vmem_limit_bytes=60 * 1024 * 1024
        ),
    )(*args)


def solution(mesh):
    nz = mesh.shape["sp"] // NY
    nx = mesh.shape["tp"] // 2
    in_specs = (
        P(("sp", "tp"), None),
        P(("sp", "tp"), None),
        P(),
        P(),
        P(None, None, "tp"),
        P(None, None, "tp"),
        P(None, None, "tp"),
        P(None, "tp"),
        P(None, "tp", None),
        P(),
        P(None, "tp"),
        P(None, "tp"),
        P("tp", None),
    )
    out_specs = P(("sp", "tp"), None)
    return jax.shard_map(
        functools.partial(local, nz, nx),
        mesh=mesh,
        in_specs=in_specs,
        out_specs=out_specs,
        check_vma=False,
    )
```

```python
import functools
import math

import jax
import jax.numpy as jnp
from jax import lax
from jax.experimental import pallas as pl
from jax.experimental.pallas import tpu as pltpu
from jax.sharding import PartitionSpec as P

HEAD_DIM = 128
EPSILON = 1e-06
NY = 4
MESH = pl.DeviceIdType.MESH
BF16 = jnp.bfloat16
F32 = jnp.float32


def rcopy(src, dst, send, recv, peer):
    return pltpu.make_async_remote_copy(
        src_ref=src,
        dst_ref=dst,
        send_sem=send,
        recv_sem=recv,
        device_id=peer,
        device_id_type=MESH,
    )


def at(index, size):
    return pl.ds(pl.multiple_of(index * size, size), size)


def body(
    nz,
    nx,
    source,
    target,
    source_gain,
    target_gain,
    query_weight,
    key_weight,
    value_weight,
    head_gain,
    out_weight,
    mlp_gain,
    gate_weight,
    up_weight,
    down_weight,
    out,
    src,
    tgt,
    wkv,
    wq,
    sgain,
    tgain,
    mgain,
    hgain,
    wo,
    wg,
    wu,
    wd,
    normed,
    kb,
    vb,
    qb,
    score,
    po,
    ps,
    pr,
    prs,
    ho,
    st,
    hid,
    part,
    pb,
    d2,
    comb,
    fr,
    mixed,
    lsem,
    src_s,
    src_r,
    ag_s,
    ag_r,
    w_s,
    w_r,
    k_s,
    k_r,
    k0_r,
    q_s,
    q_r,
    p_s,
    p_r,
    d_s,
    d_r,
    f_s,
    f_r,
    o_s,
):
    ntp = 2 * nx
    depth = src.shape[1]
    src_rows = src.shape[0] // ntp
    own_rows = tgt.shape[0] // ntp
    rows = tgt.shape[0]
    block = src.shape[0]
    chunk = 2 * src_rows
    cols = depth // ntp
    hd = HEAD_DIM
    sp = lax.axis_index("sp")
    tp = lax.axis_index("tp")
    z = lax.div(sp, NY)
    y = lax.rem(sp, NY)
    x = lax.div(tp, 2)
    c = lax.rem(tp, 2)

    def device(zz, yy, xx, cc):
        return (zz * NY + yy, xx * 2 + cc)

    def x_peer(d):
        return device(z, y, lax.rem(x + d, nx), c)

    def y_peer(d):
        return device(z, lax.rem(y + d, NY), x, c)

    def z_peer(d):
        return device(lax.rem(z + d, nz), y, x, c)

    partner = device(z, y, x, 1 - c)
    x_order = (1, 3, 2)
    far_first = (2, 1, 3)

    loads = {}

    def load(name, index, source_ref, to):
        loads[name] = pltpu.make_async_copy(source_ref, to, lsem.at[index])
        loads[name].start()

    load("tgt", 0, target, tgt.at[at(tp, own_rows)])
    load("src", 1, source, src.at[at(tp, src_rows)])
    load("sgain", 2, source_gain, sgain)
    load("k", 3, key_weight, wkv.at[:, :, 0:hd])
    load("v", 4, value_weight, wkv.at[:, :, hd : 2 * hd])
    load("tgain", 5, target_gain, tgain)
    load("q", 6, query_weight, wq)
    load("hgain", 7, head_gain, hgain)
    load("mgain", 8, mlp_gain, mgain)
    load("wo0", 9, out_weight.at[0], wo.at[0, at(tp, hd)])
    load("wo1", 13, out_weight.at[1], wo.at[1, at(tp, hd)])
    load("wg", 10, gate_weight, wg)
    load("wu", 11, up_weight, wu)
    load("wd", 12, down_weight, wd)

    scope = jax.named_scope
    barrier = pltpu.get_barrier_semaphore()
    peers = [device(z, y, lax.rem(x + d // 2, nx), lax.rem(c + d, 2)) for d in range(1, ntp)]
    peers += [y_peer(d) for d in range(1, NY)]
    peers += [z_peer(d) for d in range(1, nz)]
    with scope("barrier"):
        for peer in peers:
            pl.semaphore_signal(barrier, inc=1, device_id=peer, device_id_type=MESH)
        pl.semaphore_wait(barrier, len(peers))

    def all_sent(ref, sem):
        rcopy(ref, ref, sem, sem, partner).wait_send()

    def all_here(ref, sem):
        rcopy(ref, ref, sem, sem, partner).wait_recv()

    class Gather:
        def __init__(self, index, view):
            self.view = view
            self.send = ag_s.at[index]
            self.near = ag_r.at[index, 0]
            mine = view(tp)
            self.first = {d: rcopy(mine, mine, self.send, ag_r.at[index, d], x_peer(d)) for d in x_order}
            rcopy(mine, mine, self.send, self.near, partner).start()
            for d in far_first:
                self.first[d].start()

        def forward(self):
            for d in x_order:
                self.first[d].wait_recv()
                there = self.view(lax.rem(x + nx - d, nx) * 2 + c)
                rcopy(there, there, self.send, self.near, partner).start()

        def finish(self, near_bytes, sent_bytes):
            all_here(near_bytes, self.near)
            all_sent(sent_bytes, self.send)

    left, right = x_peer(nx - 1), x_peer(1)
    tp_left = lax.rem(x + nx - 1, nx) * 2 + c
    tp_right = lax.rem(x + 1, nx) * 2 + c
    tp_far = lax.rem(x + 2, nx) * 2 + c

    class Spread:
        def __init__(self, ref, size, send, recv, near):
            self.ref, self.size, self.half = ref, size, size // 2
            self.send, self.recv, self.near = send, recv, near

        def copy(self, sem, owner, first, count, to):
            start = pl.multiple_of(owner * self.size + first, self.half)
            ref = self.ref.at[pl.ds(start, count)]
            rcopy(ref, ref, self.send, sem, to).start()

        def wait(self, index):
            all_here(self.ref.at[pl.ds(0, self.half)], self.recv.at[index])

        def start(self):
            half = self.half
            self.copy(self.near[0], tp, 0, self.size, partner)
            self.copy(self.recv.at[1], tp, 0, half, right)
            self.copy(self.recv.at[2], tp, half, half, left)
            self.copy(self.recv.at[3], tp, half, half, right)
            self.copy(self.recv.at[4], tp, 0, half, left)

        def relay(self):
            self.wait(1)
            self.copy(self.recv.at[5], tp_left, 0, self.half, right)
            self.wait(2)
            self.copy(self.recv.at[6], tp_right, self.half, self.half, left)

        def forward_sides(self):
            self.wait(3)
            self.copy(self.near[1], tp_left, 0, self.size, partner)
            self.wait(4)
            self.copy(self.near[2], tp_right, 0, self.size, partner)

        def forward_far(self):
            self.wait(5)
            self.copy(self.near[3], tp_far, 0, self.half, partner)
            self.wait(6)
            self.copy(self.near[4], tp_far, self.half, self.half, partner)

        def sent(self):
            all_sent(self.ref.at[0 : 7 * self.size], self.send)

    spread_src = Spread(src, src_rows, src_s, src_r, [src_r.at[i] for i in (0, 7, 8, 9, 10)])
    spread_wo = [
        Spread(wo.at[layer], hd, w_s.at[layer], w_r.at[layer], [w_r.at[layer, 0]] * 5)
        for layer in range(2)
    ]
    loads["src"].wait()
    spread_src.start()

    def src_here(index, count):
        all_here(src.at[pl.ds(0, count)], src_r.at[index])

    factor = math.log2(math.e) * hd**-0.5

    def norm_rows(from_ref, start, count, gain_of):
        step = 64

        def one(i, carry):
            at_from = pl.ds(pl.multiple_of(start + i * step, step), step)
            at_to = pl.ds(pl.multiple_of(i * step, step), step)
            total = jnp.zeros((step, 128), F32)
            for k in range(0, depth, 128):
                v = from_ref[at_from, k : k + 128].astype(F32)
                total += v * v
            mean = jnp.sum(total, axis=1, keepdims=True) * (1.0 / depth)
            scale = lax.rsqrt(mean + EPSILON)
            for k in range(0, depth, 128):
                v = from_ref[at_from, k : k + 128].astype(F32)
                g = gain_of(k).astype(F32)
                normed[at_to, k : k + 128] = (v * scale * g).astype(BF16)
            return carry

        lax.fori_loop(0, count // step, one, 0)

    def project_source(layer, xx):
        norm_rows(src, xx * chunk, chunk, lambda k: sgain[layer : layer + 1, k : k + 128])
        kv = jnp.dot(normed[0:chunk], wkv[layer], preferred_element_type=F32)
        first = y * block + xx * chunk
        here = pl.ds(pl.multiple_of(first, chunk), chunk)
        kb[layer, here] = kv[:, 0:hd].astype(BF16)
        vb[layer, :, here] = jnp.transpose(kv[:, hd : 2 * hd]).astype(BF16)

    def k0_copy(kind, yy, xx, recv, to):
        here = pl.ds(pl.multiple_of(yy * block + xx * chunk, chunk), chunk)
        ref = vb.at[0, :, here] if kind else kb.at[0, here]
        return rcopy(ref, ref, k_s.at[0, kind], recv, to)

    def send_k0(xx):
        after, before = y_peer(1), y_peer(NY - 1)
        k0_copy(0, y, xx, k0_r.at[0, xx], after).start()
        k0_copy(1, y, xx, k0_r.at[1, xx], before).start()
        k0_copy(0, y, xx, k_r.at[0, 0], before).start()
        k0_copy(1, y, xx, k_r.at[0, 1], after).start()

    def relay_k0(xx):
        after, before = y_peer(1), y_peer(NY - 1)
        k0_copy(0, y, xx, k0_r.at[0, xx], after).wait_recv()
        k0_copy(0, lax.rem(y + NY - 1, NY), xx, k_r.at[0, 0], after).start()
        k0_copy(1, y, xx, k0_r.at[1, xx], before).wait_recv()
        k0_copy(1, lax.rem(y + 1, NY), xx, k_r.at[0, 1], before).start()

    def k1_copies(d):
        here = at(y, block)
        k = kb.at[1, here]
        v = vb.at[1, :, here]
        return (
            rcopy(k, k, k_s.at[1, 0], k_r.at[1, 0], y_peer(d)),
            rcopy(v, v, k_s.at[1, 1], k_r.at[1, 1], y_peer(d)),
        )

    def z_order(i):
        odd = lax.rem(i, 2)
        return odd * lax.div(i + 1, 2) + (1 - odd) * lax.rem(nz - lax.div(i, 2), nz)

    def q_copy(layer, slot, source_slot=0, d=None):
        to = z_peer(z_order(slot) if d is None else d)
        return rcopy(
            qb.at[layer, source_slot],
            qb.at[layer, slot],
            q_s.at[layer],
            q_r.at[layer, slot],
            to,
        )

    def project_query(layer, state_ref):
        norm_rows(state_ref, 0, rows, lambda k: tgain[layer : layer + 1, k : k + 128])
        q = jnp.dot(normed[0:rows], wq[layer], preferred_element_type=F32)
        qb[layer, 0] = (q * factor).astype(BF16)

        for slot in (3, 4, 1, 2):
            q_copy(layer, slot).start()

    def q_wait(layer, slot):
        q_copy(layer, slot).wait_recv()

    def relay_queries(layer):
        q_wait(layer, 3)
        q_copy(layer, 5, 3, 1).start()
        q_wait(layer, 4)
        q_copy(layer, 6, 4, nz - 1).start()
        q_copy(layer, 7, 3 + c, 2 + c * (nz - 4)).start()

    with scope("wait_own"):
        loads["sgain"].wait()
        loads["k"].wait()
        loads["v"].wait()
        src_here(0, src_rows)
    with scope("kv_own"):
        project_source(0, x)
        send_k0(x)
    with scope("wait_src"):
        spread_src.relay()
        loads["tgt"].wait()
        gather_tgt = Gather(0, lambda j: tgt.at[at(j, own_rows)])
        spread_src.forward_sides()
        src_here(7, src_rows)
    x_left, x_right, x_far = (lax.rem(x + d, nx) for d in (nx - 1, 1, 2))
    with scope("relay_k0"):
        relay_k0(x)
    with scope("kv_left"):
        project_source(0, x_left)
        send_k0(x_left)
    src_here(8, src_rows)
    with scope("kv_right"):
        project_source(0, x_right)
        send_k0(x_right)
    with scope("wait_far"):
        spread_src.forward_far()
        src_here(9, src_rows // 2)
        src_here(10, src_rows // 2)
    with scope("pass_tgt"):
        gather_tgt.forward()
    loads["wo0"].wait()
    spread_wo[0].start()
    with scope("kv_far"):
        project_source(0, x_far)
        send_k0(x_far)
    with scope("wait_tgt"):
        gather_tgt.finish(tgt.at[0 : 4 * own_rows], tgt.at[0 : 7 * own_rows])
        loads["tgain"].wait()
        loads["q"].wait()
    with scope("q0"):
        project_query(0, tgt)
    with scope("relay_k0"):
        relay_k0(x_left)
        relay_k0(x_right)

    def project_one(i, carry):
        project_source(1, i)
        return carry

    with scope("kv1"):
        lax.fori_loop(0, nx // 2, project_one, 0)
    with scope("relay_k0"):
        relay_k0(x_far)
    with scope("kv1"):
        lax.fori_loop(nx // 2, nx, project_one, 0)
    with scope("relay_q0"):
        relay_queries(0)
    for d in (1, 3, 2):
        for cp in k1_copies(d):
            cp.start()

    def p_copies(layer, slot):
        to = z_peer(nz - z_order(slot))
        return (
            rcopy(
                po.at[layer, slot], pr.at[layer, slot], p_s.at[layer, 0], p_r.at[layer, 0], to
            ),
            rcopy(
                ps.at[layer, slot], prs.at[layer, slot], p_s.at[layer, 1], p_r.at[layer, 1], to
            ),
        )

    def attend(layer, first, count):
        wide = count * rows
        q = qb[layer, pl.ds(first, count)].reshape(wide, hd)
        top = None
        for b in range(NY):
            here = slice(b * block, (b + 1) * block)
            s = lax.dot_general(
                kb[layer, here], q, (((1,), (1,)), ((), ())), preferred_element_type=F32
            )
            score[here, 0:wide] = s
            m = jnp.max(s, axis=0, keepdims=True)
            top = m if top is None else jnp.maximum(top, m)
        total = jnp.zeros((1, wide), F32)
        acc = jnp.zeros((hd, wide), F32)
        for b in range(NY):
            here = slice(b * block, (b + 1) * block)
            w = jnp.exp2(score[here, 0:wide] - top)
            total += jnp.sum(w, axis=0, keepdims=True)
            acc += jnp.dot(vb[layer, :, here], w.astype(BF16), preferred_element_type=F32)
        low = acc.astype(BF16)
        which = lax.broadcasted_iota(jnp.int32, (8, wide), 0)
        stats = jnp.where(which == 0, top, total)
        for j in range(count):
            to_out, to_stats = (pr, prs) if isinstance(first, int) and first == 0 else (po, ps)
            to_out[layer, first + j] = low[:, j * rows : (j + 1) * rows]
            to_stats[layer, first + j] = stats[:, j * rows : (j + 1) * rows]
            if to_out is po:
                for cp in p_copies(layer, first + j):
                    cp.start()

    def attend_first():
        attend(0, 3, 2)
        q_wait(0, 1)
        q_wait(0, 2)
        attend(0, 1, 2)
        with scope("wait_q"):
            q_wait(0, 7)
        attend(0, 7, 1)
        q_wait(0, 5)
        q_wait(0, 6)
        attend(0, 5, 2)
        attend(0, 0, 1)

    def attend_second():
        attend(1, 0, 1)
        with scope("relay_q1"):
            relay_queries(1)
        with scope("wait_q"):
            q_wait(1, 1)
            q_wait(1, 2)
        attend(1, 1, 2)
        attend(1, 3, 2)
        with scope("relay_wo1"):
            spread_wo[1].relay()
        with scope("wait_q"):
            q_wait(1, 7)
        attend(1, 7, 1)
        with scope("wait_q"):
            q_wait(1, 5)
            q_wait(1, 6)
        attend(1, 5, 2)

    def merge(layer):
        with scope("wait_p"):
            all_here(pr.at[layer, 1:nz], p_r.at[layer, 0])
            all_here(prs.at[layer, 1:nz], p_r.at[layer, 1])
        top = prs[layer, 0, 0:1]
        for d in range(1, nz):
            top = jnp.maximum(top, prs[layer, d, 0:1])
        total = jnp.zeros((1, rows), F32)
        acc = jnp.zeros((hd, rows), F32)
        for d in range(nz):
            f = jnp.exp2(prs[layer, d, 0:1] - top)
            total += f * prs[layer, d, 1:2]
            acc += f * pr[layer, d].astype(F32)
        attended = acc / total
        mean = jnp.mean(attended * attended, axis=0, keepdims=True)
        scaled = jnp.transpose(attended * lax.rsqrt(mean + EPSILON))
        gain = hgain[layer : layer + 1, :].astype(F32)
        ho[layer, :, at(tp, hd)] = (scaled * gain).astype(BF16)

    def gather_heads(layer):
        with scope("gather_ho"):
            send, recv = ag_s.at[1 + layer], ag_r.at[1 + layer, 0]
            mine = ho.at[layer, :, at(tp, hd)]
            for d in (4, 5, 2, 3, 6, 7, 1):
                to = device(z, y, lax.rem(x + d // 2, nx), lax.rem(c + d, 2))
                rcopy(mine, mine, send, recv, to).start()
            spread_wo[layer].forward_far()
            seven = ho.at[layer, :, 0 : 7 * hd]
            all_here(seven, recv)
            all_sent(seven, send)

    def project_heads(layer, old):
        with scope("wait_wo"):
            all_here(wo.at[layer, 0 : 4 * hd], w_r.at[layer, 0])
        with scope("out"):

            def out_piece(i, carry):
                w = at(i, 512)
                add = jnp.dot(ho[layer], wo[layer, :, w], preferred_element_type=F32)
                st[layer, :, w] = (old[:, w].astype(F32) + add).astype(BF16)
                return carry

            lax.fori_loop(0, depth // 512, out_piece, 0)

    def kv_wait(layer):
        most = (NY - 1 - (layer == 0)) * block
        all_here(kb.at[layer, 0:most], k_r.at[layer, 0])
        all_here(vb.at[layer, :, 0:most], k_r.at[layer, 1])

    with scope("wait_kv0"):
        kv_wait(0)
    with scope("relay_wo0"):
        spread_wo[0].relay()
    with scope("attend0"):
        attend_first()
    with scope("sides_wo0"):
        spread_wo[0].forward_sides()
    loads["hgain"].wait()
    with scope("merge0"):
        merge(0)
    gather_heads(0)
    loads["wo1"].wait()
    spread_wo[1].start()
    project_heads(0, tgt)
    with scope("q1"):
        project_query(1, st.at[0])
    with scope("wait_kv1"):
        kv_wait(1)
    with scope("attend1"):
        attend_second()
    with scope("sides_wo1"):
        spread_wo[1].forward_sides()
    with scope("merge1"):
        merge(1)
    gather_heads(1)
    project_heads(1, st.at[0])

    loads["mgain"].wait()
    loads["wg"].wait()
    loads["wu"].wait()
    loads["wd"].wait()
    with scope("mlp_norm"):
        norm_rows(st.at[1], 0, rows, lambda k: mgain[k // 128 : k // 128 + 1, :])
    over = (((1,), (1,)), ((), ()))
    with scope("gate"):
        gate = lax.dot_general(wg[...], normed[0:rows], over, preferred_element_type=F32)
        up = lax.dot_general(wu[...], normed[0:rows], over, preferred_element_type=F32)
        hid[...] = jnp.transpose(gate / (1.0 + jnp.exp(-gate)) * up).astype(BF16)
    pieces = 4
    width = depth // pieces

    def d2_copy(n):
        w = slice(n * width, (n + 1) * width)
        return rcopy(pb.at[:, :, w], d2.at[:, :, w], d_s, d_r.at[n], partner)

    def fr_copy(n, d):
        w = slice(n * width, (n + 1) * width)
        return rcopy(comb.at[d, :, w], fr.at[d, :, w], f_s, f_r.at[n], x_peer(d))

    def pair_sum(n):
        w = slice(n * width, (n + 1) * width)
        with scope("wait_d2"):
            d2_copy(n).wait_recv()
        for d in far_first:
            xx = lax.rem(x + d, nx)
            comb[d, :, w] = (part[xx, c, :, w] + d2[xx, :, w].astype(F32)).astype(BF16)
            fr_copy(n, d).start()

    for n in range(pieces):
        w = slice(n * width, (n + 1) * width)
        with scope("down"):
            down = jnp.dot(hid[...], wd[:, w], preferred_element_type=F32)
            part[:, :, :, w] = down.reshape(nx, 2, own_rows, width)
            pb[:, :, w] = part[:, 1 - c, :, w].astype(BF16)
            d2_copy(n).start()
    for n in range(pieces):
        pair_sum(n)
    def out_piece_copy(n):
        w = slice(n * width, (n + 1) * width)
        return pltpu.make_async_copy(mixed.at[:, w], out.at[:, w], o_s)

    for n in range(pieces):
        w = slice(n * width, (n + 1) * width)
        down = part[x, c, :, w] + d2[x, :, w].astype(F32)
        with scope("wait_fr"):
            all_here(fr.at[1:nx, :, w], f_r.at[n])
        for d in x_order:
            down += fr[d, :, w].astype(F32)
        state = st[1, at(tp, own_rows), w].astype(F32)
        mixed[:, w] = (state + 0.5 * down).astype(BF16)
        out_piece_copy(n).start()

    with scope("drain"):
        spread_src.sent()
        for spread in spread_wo:
            spread.sent()
        for layer in range(2):
            all_sent(kb.at[layer, 0 : (NY - 1) * block], k_s.at[layer, 0])
            all_sent(vb.at[layer, :, 0 : (NY - 1) * block], k_s.at[layer, 1])
            all_sent(qb.at[layer, 1:nz], q_s.at[layer])
            all_sent(po.at[layer, 1:nz], p_s.at[layer, 0])
            all_sent(ps.at[layer, 1:nz], p_s.at[layer, 1])
        all_sent(pb, d_s)
        all_sent(comb.at[1:nx], f_s)
        pltpu.make_async_copy(mixed, out, o_s).wait()


def local(nz, nx, *args):
    source, target = args[0], args[1]
    ntp = 2 * nx
    depth = source.shape[1]
    block = source.shape[0] * ntp
    rows = target.shape[0] * ntp
    own = target.shape[0]
    ffl = args[10].shape[1]
    hd = HEAD_DIM
    args = list(args)
    args[9] = args[9].reshape(depth // 128, 128)
    args[10] = args[10].T
    args[11] = args[11].T
    vmem = pltpu.VMEM
    dma = pltpu.SemaphoreType.DMA
    scratch = [
        vmem((block, depth), BF16),
        vmem((rows, depth), BF16),
        vmem((2, depth, 2 * hd), BF16),
        vmem((2, depth, hd), BF16),
        vmem((2, depth), BF16),
        vmem((2, depth), BF16),
        vmem((depth // 128, 128), BF16),
        vmem((2, hd), BF16),
        vmem((2, ntp * hd, depth), BF16),
        vmem((ffl, depth), BF16),
        vmem((ffl, depth), BF16),
        vmem((ffl, depth), BF16),
        vmem((rows, depth), BF16),
        vmem((2, NY * block, hd), BF16),
        vmem((2, hd, NY * block), BF16),
        vmem((2, nz, rows, hd), BF16),
        vmem((NY * block, 2 * rows), F32),
        vmem((2, nz, hd, rows), BF16),
        vmem((2, nz, 8, rows), F32),
        vmem((2, nz, hd, rows), BF16),
        vmem((2, nz, 8, rows), F32),
        vmem((2, rows, ntp * hd), BF16),
        vmem((2, rows, depth), BF16),
        vmem((rows, ffl), BF16),
        vmem((nx, 2, own, depth), F32),
        vmem((nx, own, depth), BF16),
        vmem((nx, own, depth), BF16),
        vmem((nx, own, depth), BF16),
        vmem((nx, own, depth), BF16),
        vmem((own, depth), BF16),
        dma((14,)),
        dma(()),
        dma((11,)),
        dma((3,)),
        dma((3, nx)),
        dma((2,)),
        dma((2, 7)),
        dma((2, 2)),
        dma((2, 2)),
        dma((2, nx)),
        dma((2,)),
        dma((2, nz)),
        dma((2, 2)),
        dma((2, 2)),
        dma(()),
        dma((4,)),
        dma(()),
        dma((4,)),
        dma(()),
    ]
    return pl.pallas_call(
        functools.partial(body, nz, nx),
        name="decoder",
        out_shape=jax.ShapeDtypeStruct(target.shape, BF16),
        in_specs=[pl.BlockSpec(memory_space=pl.ANY)] * len(args),
        out_specs=pl.BlockSpec(memory_space=pl.ANY),
        scratch_shapes=scratch,
        compiler_params=pltpu.CompilerParams(
            collective_id=0, has_side_effects=True, vmem_limit_bytes=60 * 1024 * 1024
        ),
    )(*args)


def solution(mesh):
    nz = mesh.shape["sp"] // NY
    nx = mesh.shape["tp"] // 2
    in_specs = (
        P(("sp", "tp"), None),
        P(("sp", "tp"), None),
        P(),
        P(),
        P(None, None, "tp"),
        P(None, None, "tp"),
        P(None, None, "tp"),
        P(None, "tp"),
        P(None, "tp", None),
        P(),
        P(None, "tp"),
        P(None, "tp"),
        P("tp", None),
    )
    out_specs = P(("sp", "tp"), None)
    return jax.shard_map(
        functools.partial(local, nz, nx),
        mesh=mesh,
        in_specs=in_specs,
        out_specs=out_specs,
        check_vma=False,
    )
```

```python
import functools
import math

import jax
import jax.numpy as jnp
from jax import lax
from jax.experimental import pallas as pl
from jax.experimental.pallas import tpu as pltpu
from jax.sharding import PartitionSpec as P

HEAD_DIM = 128
EPSILON = 1e-06
NY = 4
MESH = pl.DeviceIdType.MESH
BF16 = jnp.bfloat16
F32 = jnp.float32


def rcopy(src, dst, send, recv, peer):
    return pltpu.make_async_remote_copy(
        src_ref=src,
        dst_ref=dst,
        send_sem=send,
        recv_sem=recv,
        device_id=peer,
        device_id_type=MESH,
    )


def at(index, size):
    return pl.ds(pl.multiple_of(index * size, size), size)


def body(
    nz,
    nx,
    source,
    target,
    source_gain,
    target_gain,
    query_weight,
    key_weight,
    value_weight,
    head_gain,
    out_weight,
    mlp_gain,
    gate_weight,
    up_weight,
    down_weight,
    out,
    src,
    tgt,
    wkv,
    wq,
    sgain,
    tgain,
    mgain,
    hgain,
    wo,
    wg,
    wu,
    wd,
    normed,
    kb,
    vb,
    qb,
    score,
    po,
    ps,
    pr,
    prs,
    ho,
    st,
    hid,
    part,
    pb,
    d2,
    comb,
    fr,
    mixed,
    lsem,
    src_s,
    src_r,
    ag_s,
    ag_r,
    w_s,
    w_r,
    k_s,
    k_r,
    k0_r,
    q_s,
    q_r,
    p_s,
    p_r,
    d_s,
    d_r,
    f_s,
    f_r,
    o_s,
):
    ntp = 2 * nx
    depth = src.shape[1]
    src_rows = src.shape[0] // ntp
    own_rows = tgt.shape[0] // ntp
    rows = tgt.shape[0]
    block = src.shape[0]
    chunk = 2 * src_rows
    cols = depth // ntp
    hd = HEAD_DIM
    sp = lax.axis_index("sp")
    tp = lax.axis_index("tp")
    z = lax.div(sp, NY)
    y = lax.rem(sp, NY)
    x = lax.div(tp, 2)
    c = lax.rem(tp, 2)

    def device(zz, yy, xx, cc):
        return (zz * NY + yy, xx * 2 + cc)

    def x_peer(d):
        return device(z, y, lax.rem(x + d, nx), c)

    def y_peer(d):
        return device(z, lax.rem(y + d, NY), x, c)

    def z_peer(d):
        return device(lax.rem(z + d, nz), y, x, c)

    partner = device(z, y, x, 1 - c)
    x_order = (1, 3, 2)
    far_first = (2, 1, 3)

    loads = {}

    def load(name, index, source_ref, to):
        loads[name] = pltpu.make_async_copy(source_ref, to, lsem.at[index])
        loads[name].start()

    load("tgt", 0, target, tgt.at[at(tp, own_rows)])
    load("src", 1, source, src.at[at(tp, src_rows)])
    load("sgain", 2, source_gain, sgain)
    load("k", 3, key_weight, wkv.at[:, :, 0:hd])
    load("v", 4, value_weight, wkv.at[:, :, hd : 2 * hd])
    load("tgain", 5, target_gain, tgain)
    load("q", 6, query_weight, wq)
    load("hgain", 7, head_gain, hgain)
    load("mgain", 8, mlp_gain, mgain)
    load("wo0", 9, out_weight.at[0], wo.at[0, at(tp, hd)])
    load("wo1", 13, out_weight.at[1], wo.at[1, at(tp, hd)])
    load("wg", 10, gate_weight, wg)
    load("wu", 11, up_weight, wu)
    load("wd", 12, down_weight, wd)

    scope = jax.named_scope
    barrier = pltpu.get_barrier_semaphore()
    peers = [device(z, y, lax.rem(x + d // 2, nx), lax.rem(c + d, 2)) for d in range(1, ntp)]
    peers += [y_peer(d) for d in range(1, NY)]
    peers += [z_peer(d) for d in range(1, nz)]
    with scope("barrier"):
        for peer in peers:
            pl.semaphore_signal(barrier, inc=1, device_id=peer, device_id_type=MESH)
        pl.semaphore_wait(barrier, len(peers))

    def all_sent(ref, sem):
        rcopy(ref, ref, sem, sem, partner).wait_send()

    def all_here(ref, sem):
        rcopy(ref, ref, sem, sem, partner).wait_recv()

    class Gather:
        def __init__(self, index, view):
            self.view = view
            self.send = ag_s.at[index]
            self.near = ag_r.at[index, 0]
            mine = view(tp)
            self.first = {d: rcopy(mine, mine, self.send, ag_r.at[index, d], x_peer(d)) for d in x_order}
            rcopy(mine, mine, self.send, self.near, partner).start()
            for d in far_first:
                self.first[d].start()

        def forward(self):
            for d in x_order:
                self.first[d].wait_recv()
                there = self.view(lax.rem(x + nx - d, nx) * 2 + c)
                rcopy(there, there, self.send, self.near, partner).start()

        def finish(self, near_bytes, sent_bytes):
            all_here(near_bytes, self.near)
            all_sent(sent_bytes, self.send)

    left, right = x_peer(nx - 1), x_peer(1)
    tp_left = lax.rem(x + nx - 1, nx) * 2 + c
    tp_right = lax.rem(x + 1, nx) * 2 + c
    tp_far = lax.rem(x + 2, nx) * 2 + c

    class Spread:
        def __init__(self, ref, size, send, recv, near):
            self.ref, self.size, self.half = ref, size, size // 2
            self.send, self.recv, self.near = send, recv, near

        def copy(self, sem, owner, first, count, to):
            start = pl.multiple_of(owner * self.size + first, self.half)
            ref = self.ref.at[pl.ds(start, count)]
            rcopy(ref, ref, self.send, sem, to).start()

        def wait(self, index):
            all_here(self.ref.at[pl.ds(0, self.half)], self.recv.at[index])

        def start(self):
            half = self.half
            self.copy(self.near[0], tp, 0, self.size, partner)
            self.copy(self.recv.at[1], tp, 0, half, right)
            self.copy(self.recv.at[2], tp, half, half, left)
            self.copy(self.recv.at[3], tp, half, half, right)
            self.copy(self.recv.at[4], tp, 0, half, left)

        def relay(self):
            self.wait(1)
            self.copy(self.recv.at[5], tp_left, 0, self.half, right)
            self.copy(self.near[1], tp_left, 0, self.half, partner)
            self.wait(2)
            self.copy(self.recv.at[6], tp_right, self.half, self.half, left)
            self.copy(self.near[2], tp_right, self.half, self.half, partner)

        def forward_sides(self):
            self.wait(3)
            self.copy(self.near[1], tp_left, self.half, self.half, partner)
            self.wait(4)
            self.copy(self.near[2], tp_right, 0, self.half, partner)

        def forward_far(self):
            self.wait(5)
            self.copy(self.near[3], tp_far, 0, self.half, partner)
            self.wait(6)
            self.copy(self.near[4], tp_far, self.half, self.half, partner)

        def sent(self):
            all_sent(self.ref.at[0 : 7 * self.size], self.send)

    spread_src = Spread(src, src_rows, src_s, src_r, [src_r.at[i] for i in (0, 7, 8, 9, 10)])
    spread_wo = [
        Spread(wo.at[layer], hd, w_s.at[layer], w_r.at[layer], [w_r.at[layer, 0]] * 5)
        for layer in range(2)
    ]
    loads["src"].wait()
    spread_src.start()

    def src_here(index, count):
        all_here(src.at[pl.ds(0, count)], src_r.at[index])

    factor = math.log2(math.e) * hd**-0.5

    def norm_rows(from_ref, start, count, gain_of):
        step = 64

        def one(i, carry):
            at_from = pl.ds(pl.multiple_of(start + i * step, step), step)
            at_to = pl.ds(pl.multiple_of(i * step, step), step)
            total = jnp.zeros((step, 128), F32)
            for k in range(0, depth, 128):
                v = from_ref[at_from, k : k + 128].astype(F32)
                total += v * v
            mean = jnp.sum(total, axis=1, keepdims=True) * (1.0 / depth)
            scale = lax.rsqrt(mean + EPSILON)
            for k in range(0, depth, 128):
                v = from_ref[at_from, k : k + 128].astype(F32)
                g = gain_of(k).astype(F32)
                normed[at_to, k : k + 128] = (v * scale * g).astype(BF16)
            return carry

        lax.fori_loop(0, count // step, one, 0, unroll=True)

    def project_source(layer, xx):
        norm_rows(src, xx * chunk, chunk, lambda k: sgain[layer : layer + 1, k : k + 128])
        kv = jnp.dot(normed[0:chunk], wkv[layer], preferred_element_type=F32)
        first = y * block + xx * chunk
        here = pl.ds(pl.multiple_of(first, chunk), chunk)
        kb[layer, here] = kv[:, 0:hd].astype(BF16)
        vb[layer, :, here] = jnp.transpose(kv[:, hd : 2 * hd]).astype(BF16)

    def k0_copy(kind, yy, xx, recv, to):
        here = pl.ds(pl.multiple_of(yy * block + xx * chunk, chunk), chunk)
        ref = vb.at[0, :, here] if kind else kb.at[0, here]
        return rcopy(ref, ref, k_s.at[0, kind], recv, to)

    def send_k0(xx):
        after, before = y_peer(1), y_peer(NY - 1)
        k0_copy(0, y, xx, k0_r.at[0, xx], after).start()
        k0_copy(1, y, xx, k0_r.at[1, xx], before).start()
        k0_copy(0, y, xx, k_r.at[0, 0], before).start()
        k0_copy(1, y, xx, k_r.at[0, 1], after).start()

    def relay_k0(xx):
        after, before = y_peer(1), y_peer(NY - 1)
        k0_copy(0, y, xx, k0_r.at[0, xx], after).wait_recv()
        k0_copy(0, lax.rem(y + NY - 1, NY), xx, k_r.at[0, 0], after).start()
        k0_copy(1, y, xx, k0_r.at[1, xx], before).wait_recv()
        k0_copy(1, lax.rem(y + 1, NY), xx, k_r.at[0, 1], before).start()

    def k1_copies(d):
        here = at(y, block)
        k = kb.at[1, here]
        v = vb.at[1, :, here]
        return (
            rcopy(k, k, k_s.at[1, 0], k_r.at[1, 0], y_peer(d)),
            rcopy(v, v, k_s.at[1, 1], k_r.at[1, 1], y_peer(d)),
        )

    def z_order(i):
        odd = lax.rem(i, 2)
        return odd * lax.div(i + 1, 2) + (1 - odd) * lax.rem(nz - lax.div(i, 2), nz)

    def q_copy(layer, slot, source_slot=0, d=None):
        to = z_peer(z_order(slot) if d is None else d)
        return rcopy(
            qb.at[layer, source_slot],
            qb.at[layer, slot],
            q_s.at[layer],
            q_r.at[layer, slot],
            to,
        )

    def project_query(layer, state_ref):
        norm_rows(state_ref, 0, rows, lambda k: tgain[layer : layer + 1, k : k + 128])
        q = jnp.dot(normed[0:rows], wq[layer], preferred_element_type=F32)
        qb[layer, 0] = (q * factor).astype(BF16)

        for slot in (3, 4, 1, 2):
            q_copy(layer, slot).start()

    def q_wait(layer, slot):
        q_copy(layer, slot).wait_recv()

    def relay_queries(layer):
        q_wait(layer, 3)
        q_copy(layer, 5, 3, 1).start()
        q_wait(layer, 4)
        q_copy(layer, 6, 4, nz - 1).start()
        q_copy(layer, 7, 3 + c, 2 + c * (nz - 4)).start()

    with scope("wait_own"):
        loads["sgain"].wait()
        loads["k"].wait()
        loads["v"].wait()
        src_here(0, src_rows)
    with scope("kv_own"):
        project_source(0, x)
        send_k0(x)
    with scope("wait_src"):
        spread_src.relay()
        loads["tgt"].wait()
        gather_tgt = Gather(0, lambda j: tgt.at[at(j, own_rows)])
        spread_src.forward_sides()
        src_here(7, src_rows)
    x_left, x_right, x_far = (lax.rem(x + d, nx) for d in (nx - 1, 1, 2))
    with scope("relay_k0"):
        relay_k0(x)
    with scope("kv_left"):
        project_source(0, x_left)
        send_k0(x_left)
    src_here(8, src_rows)
    with scope("kv_right"):
        project_source(0, x_right)
        send_k0(x_right)
    with scope("wait_far"):
        spread_src.forward_far()
        src_here(9, src_rows // 2)
        src_here(10, src_rows // 2)
    with scope("pass_tgt"):
        gather_tgt.forward()
    loads["wo0"].wait()
    spread_wo[0].start()
    with scope("kv_far"):
        project_source(0, x_far)
        send_k0(x_far)
    with scope("wait_tgt"):
        gather_tgt.finish(tgt.at[0 : 4 * own_rows], tgt.at[0 : 7 * own_rows])
        loads["tgain"].wait()
        loads["q"].wait()
    with scope("q0"):
        project_query(0, tgt)
    with scope("relay_k0"):
        relay_k0(x_left)
        relay_k0(x_right)

    def project_one(i, carry):
        project_source(1, i)
        return carry

    with scope("kv1"):
        lax.fori_loop(0, nx // 2, project_one, 0)
    with scope("relay_k0"):
        relay_k0(x_far)
    with scope("kv1"):
        lax.fori_loop(nx // 2, nx, project_one, 0)
    with scope("relay_q0"):
        relay_queries(0)
    for d in (1, 3, 2):
        for cp in k1_copies(d):
            cp.start()

    def p_copies(layer, slot):
        to = z_peer(nz - z_order(slot))
        return (
            rcopy(
                po.at[layer, slot], pr.at[layer, slot], p_s.at[layer, 0], p_r.at[layer, 0], to
            ),
            rcopy(
                ps.at[layer, slot], prs.at[layer, slot], p_s.at[layer, 1], p_r.at[layer, 1], to
            ),
        )

    def attend(layer, first, count):
        wide = count * rows
        q = qb[layer, pl.ds(first, count)].reshape(wide, hd)
        top = None
        for b in range(NY):
            here = slice(b * block, (b + 1) * block)
            s = lax.dot_general(
                kb[layer, here], q, (((1,), (1,)), ((), ())), preferred_element_type=F32
            )
            score[here, 0:wide] = s
            m = jnp.max(s, axis=0, keepdims=True)
            top = m if top is None else jnp.maximum(top, m)
        total = jnp.zeros((1, wide), F32)
        acc = jnp.zeros((hd, wide), F32)
        for b in range(NY):
            here = slice(b * block, (b + 1) * block)
            w = jnp.exp2(score[here, 0:wide] - top)
            total += jnp.sum(w, axis=0, keepdims=True)
            acc += jnp.dot(vb[layer, :, here], w.astype(BF16), preferred_element_type=F32)
        low = acc.astype(BF16)
        which = lax.broadcasted_iota(jnp.int32, (8, wide), 0)
        stats = jnp.where(which == 0, top, total)
        for j in range(count):
            to_out, to_stats = (pr, prs) if isinstance(first, int) and first == 0 else (po, ps)
            to_out[layer, first + j] = low[:, j * rows : (j + 1) * rows]
            to_stats[layer, first + j] = stats[:, j * rows : (j + 1) * rows]
            if to_out is po:
                for cp in p_copies(layer, first + j):
                    cp.start()

    def attend_first():
        attend(0, 3, 2)
        attend(0, 0, 1)
        with scope("wait_q"):
            q_wait(0, 7)
        attend(0, 7, 1)
        q_wait(0, 5)
        q_wait(0, 6)
        attend(0, 5, 2)
        q_wait(0, 1)
        q_wait(0, 2)
        attend(0, 1, 2)

    def attend_second():
        attend(1, 0, 1)
        with scope("relay_q1"):
            relay_queries(1)
        with scope("wait_q"):
            q_wait(1, 1)
            q_wait(1, 2)
        attend(1, 1, 2)
        attend(1, 3, 2)
        with scope("relay_wo1"):
            spread_wo[1].relay()
        with scope("wait_q"):
            q_wait(1, 7)
        attend(1, 7, 1)
        with scope("wait_q"):
            q_wait(1, 5)
            q_wait(1, 6)
        attend(1, 5, 2)

    def merge(layer):
        with scope("wait_p"):
            all_here(pr.at[layer, 1:nz], p_r.at[layer, 0])
            all_here(prs.at[layer, 1:nz], p_r.at[layer, 1])
        top = prs[layer, 0, 0:1]
        for d in range(1, nz):
            top = jnp.maximum(top, prs[layer, d, 0:1])
        total = jnp.zeros((1, rows), F32)
        acc = jnp.zeros((hd, rows), F32)
        for d in range(nz):
            f = jnp.exp2(prs[layer, d, 0:1] - top)
            total += f * prs[layer, d, 1:2]
            acc += f * pr[layer, d].astype(F32)
        attended = acc / total
        mean = jnp.mean(attended * attended, axis=0, keepdims=True)
        scaled = jnp.transpose(attended * lax.rsqrt(mean + EPSILON))
        gain = hgain[layer : layer + 1, :].astype(F32)
        ho[layer, :, at(tp, hd)] = (scaled * gain).astype(BF16)

    def gather_heads(layer):
        with scope("gather_ho"):
            send, recv = ag_s.at[1 + layer], ag_r.at[1 + layer, 0]
            mine = ho.at[layer, :, at(tp, hd)]
            for d in (4, 5, 2, 3, 6, 7, 1):
                to = device(z, y, lax.rem(x + d // 2, nx), lax.rem(c + d, 2))
                rcopy(mine, mine, send, recv, to).start()
            spread_wo[layer].forward_far()
            seven = ho.at[layer, :, 0 : 7 * hd]
            all_here(seven, recv)
            all_sent(seven, send)

    def project_heads(layer, old):
        with scope("wait_wo"):
            all_here(wo.at[layer, 0 : 4 * hd], w_r.at[layer, 0])
        with scope("out"):

            def out_piece(i, carry):
                w = at(i, 1024)
                add = jnp.dot(ho[layer], wo[layer, :, w], preferred_element_type=F32)
                st[layer, :, w] = (old[:, w].astype(F32) + add).astype(BF16)
                return carry

            lax.fori_loop(0, depth // 1024, out_piece, 0)

    def kv_wait(layer):
        most = (NY - 1 - (layer == 0)) * block
        all_here(kb.at[layer, 0:most], k_r.at[layer, 0])
        all_here(vb.at[layer, :, 0:most], k_r.at[layer, 1])

    with scope("wait_kv0"):
        kv_wait(0)
    with scope("relay_wo0"):
        spread_wo[0].relay()
    with scope("attend0"):
        attend_first()
    with scope("sides_wo0"):
        spread_wo[0].forward_sides()
    loads["hgain"].wait()
    with scope("merge0"):
        merge(0)
    gather_heads(0)
    loads["wo1"].wait()
    spread_wo[1].start()
    project_heads(0, tgt)
    with scope("q1"):
        project_query(1, st.at[0])
    with scope("wait_kv1"):
        kv_wait(1)
    with scope("attend1"):
        attend_second()
    with scope("sides_wo1"):
        spread_wo[1].forward_sides()
    with scope("merge1"):
        merge(1)
    gather_heads(1)
    project_heads(1, st.at[0])

    loads["mgain"].wait()
    loads["wg"].wait()
    loads["wu"].wait()
    loads["wd"].wait()
    with scope("mlp_norm"):
        norm_rows(st.at[1], 0, rows, lambda k: mgain[k // 128 : k // 128 + 1, :])
    over = (((1,), (1,)), ((), ()))
    with scope("gate"):
        gate = lax.dot_general(wg[...], normed[0:rows], over, preferred_element_type=F32)
        up = lax.dot_general(wu[...], normed[0:rows], over, preferred_element_type=F32)
        hid[...] = jnp.transpose(gate / (1.0 + jnp.exp(-gate)) * up).astype(BF16)
    pieces = 4
    width = depth // pieces

    def d2_copy(n):
        w = slice(n * width, (n + 1) * width)
        return rcopy(pb.at[:, :, w], d2.at[:, :, w], d_s, d_r.at[n], partner)

    def fr_copy(n, d):
        w = slice(n * width, (n + 1) * width)
        return rcopy(comb.at[d, :, w], fr.at[d, :, w], f_s, f_r.at[n], x_peer(d))

    def pair_sum(n):
        w = slice(n * width, (n + 1) * width)
        with scope("wait_d2"):
            d2_copy(n).wait_recv()
        for d in far_first:
            xx = lax.rem(x + d, nx)
            comb[d, :, w] = (part[xx, c, :, w] + d2[xx, :, w].astype(F32)).astype(BF16)
            fr_copy(n, d).start()

    for n in range(pieces):
        w = slice(n * width, (n + 1) * width)
        with scope("down"):
            down = jnp.dot(hid[...], wd[:, w], preferred_element_type=F32)
            part[:, :, :, w] = down.reshape(nx, 2, own_rows, width)
            pb[:, :, w] = part[:, 1 - c, :, w].astype(BF16)
            d2_copy(n).start()
    for n in range(pieces):
        pair_sum(n)
    def out_piece_copy(n):
        w = slice(n * width, (n + 1) * width)
        return pltpu.make_async_copy(mixed.at[:, w], out.at[:, w], o_s)

    for n in range(pieces):
        w = slice(n * width, (n + 1) * width)
        down = part[x, c, :, w] + d2[x, :, w].astype(F32)
        with scope("wait_fr"):
            all_here(fr.at[1:nx, :, w], f_r.at[n])
        for d in x_order:
            down += fr[d, :, w].astype(F32)
        state = st[1, at(tp, own_rows), w].astype(F32)
        mixed[:, w] = (state + 0.5 * down).astype(BF16)
        out_piece_copy(n).start()

    with scope("drain"):
        spread_src.sent()
        for spread in spread_wo:
            spread.sent()
        for layer in range(2):
            all_sent(kb.at[layer, 0 : (NY - 1) * block], k_s.at[layer, 0])
            all_sent(vb.at[layer, :, 0 : (NY - 1) * block], k_s.at[layer, 1])
            all_sent(qb.at[layer, 1:nz], q_s.at[layer])
            all_sent(po.at[layer, 1:nz], p_s.at[layer, 0])
            all_sent(ps.at[layer, 1:nz], p_s.at[layer, 1])
        all_sent(pb, d_s)
        all_sent(comb.at[1:nx], f_s)
        pltpu.make_async_copy(mixed, out, o_s).wait()


def local(nz, nx, *args):
    source, target = args[0], args[1]
    ntp = 2 * nx
    depth = source.shape[1]
    block = source.shape[0] * ntp
    rows = target.shape[0] * ntp
    own = target.shape[0]
    ffl = args[10].shape[1]
    hd = HEAD_DIM
    args = list(args)
    args[9] = args[9].reshape(depth // 128, 128)
    args[10] = args[10].T
    args[11] = args[11].T
    vmem = pltpu.VMEM
    dma = pltpu.SemaphoreType.DMA
    scratch = [
        vmem((block, depth), BF16),
        vmem((rows, depth), BF16),
        vmem((2, depth, 2 * hd), BF16),
        vmem((2, depth, hd), BF16),
        vmem((2, depth), BF16),
        vmem((2, depth), BF16),
        vmem((depth // 128, 128), BF16),
        vmem((2, hd), BF16),
        vmem((2, ntp * hd, depth), BF16),
        vmem((ffl, depth), BF16),
        vmem((ffl, depth), BF16),
        vmem((ffl, depth), BF16),
        vmem((rows, depth), BF16),
        vmem((2, NY * block, hd), BF16),
        vmem((2, hd, NY * block), BF16),
        vmem((2, nz, rows, hd), BF16),
        vmem((NY * block, 2 * rows), F32),
        vmem((2, nz, hd, rows), BF16),
        vmem((2, nz, 8, rows), F32),
        vmem((2, nz, hd, rows), BF16),
        vmem((2, nz, 8, rows), F32),
        vmem((2, rows, ntp * hd), BF16),
        vmem((2, rows, depth), BF16),
        vmem((rows, ffl), BF16),
        vmem((nx, 2, own, depth), F32),
        vmem((nx, own, depth), BF16),
        vmem((nx, own, depth), BF16),
        vmem((nx, own, depth), BF16),
        vmem((nx, own, depth), BF16),
        vmem((own, depth), BF16),
        dma((14,)),
        dma(()),
        dma((11,)),
        dma((3,)),
        dma((3, nx)),
        dma((2,)),
        dma((2, 7)),
        dma((2, 2)),
        dma((2, 2)),
        dma((2, nx)),
        dma((2,)),
        dma((2, nz)),
        dma((2, 2)),
        dma((2, 2)),
        dma(()),
        dma((4,)),
        dma(()),
        dma((4,)),
        dma(()),
    ]
    return pl.pallas_call(
        functools.partial(body, nz, nx),
        name="decoder",
        out_shape=jax.ShapeDtypeStruct(target.shape, BF16),
        in_specs=[pl.BlockSpec(memory_space=pl.ANY)] * len(args),
        out_specs=pl.BlockSpec(memory_space=pl.ANY),
        scratch_shapes=scratch,
        compiler_params=pltpu.CompilerParams(
            collective_id=0, has_side_effects=True, vmem_limit_bytes=60 * 1024 * 1024
        ),
    )(*args)


def solution(mesh):
    nz = mesh.shape["sp"] // NY
    nx = mesh.shape["tp"] // 2
    in_specs = (
        P(("sp", "tp"), None),
        P(("sp", "tp"), None),
        P(),
        P(),
        P(None, None, "tp"),
        P(None, None, "tp"),
        P(None, None, "tp"),
        P(None, "tp"),
        P(None, "tp", None),
        P(),
        P(None, "tp"),
        P(None, "tp"),
        P("tp", None),
    )
    out_specs = P(("sp", "tp"), None)
    return jax.shard_map(
        functools.partial(local, nz, nx),
        mesh=mesh,
        in_specs=in_specs,
        out_specs=out_specs,
        check_vma=False,
    )
```
